32 devices in a mesh: grp: 1, ep: 32 (over z, y, x, core).
Axes of the slice: x: 2, y: 2, z: 4, core: 2. Of those that a mesh axis runs over, the one named last changes fastest.
Arguments:
- residual_input: bfloat16 [768, 2048], P(('grp', 'ep')), may hold values from -6 to 6
- attention_norm_gain: bfloat16 [2048], replicated, may hold values from 0.099609375 to 1.8984375
- receptance_weight: bfloat16 [2048, 1024], P(None, 'ep'), may hold values from -0.125 to 0.125
- key_weight: bfloat16 [2048, 1024], P(None, 'ep'), may hold values from -0.125 to 0.125
- value_weight: bfloat16 [2048, 1024], P(None, 'ep'), may hold values from -0.125 to 0.125
- decay_weight: bfloat16 [2048, 1024], P(None, 'ep'), may hold values from -0.125 to 0.125
- correction_rate_weight: bfloat16 [2048, 1024], P(None, 'ep'), may hold values from -0.125 to 0.125
- output_gate_weight: bfloat16 [2048, 1024], P(None, 'ep'), may hold values from -0.125 to 0.125
- decay_offset: float32 [1024], replicated, may hold values from -3 to 1
- correction_rate_offset: float32 [1024], replicated, may hold values from -1.5 to 1.5
- self_term_weight: float32 [1024], replicated, may hold values from -2 to 2
- head_read_gain: float32 [1024], replicated, may hold values from 0.1 to 1.9
- previous_state: float32 [768, 16, 4096], P(('grp', 'ep')), may hold values from -4 to 4
- attention_output_weight: bfloat16 [1024, 2048], replicated, may hold values from -0.1875 to 0.1875
- feedforward_norm_gain: bfloat16 [2048], replicated, may hold values from 0.099609375 to 1.8984375
- routes: int32 [768, 4], P('grp'), may hold values from 0 to 31, all different within a row; in each aligned block of 24 rows (0 to 23, 24 to 47, ...) at most 4 rows name the same one
- routing_weight: float32 [768, 4], P('grp'), may hold values from 0.2 to 1
- routed_gate_weight: bfloat16 [32, 2048, 512], P('ep'), may hold values from -0.125 to 0.125
- routed_up_weight: bfloat16 [32, 2048, 512], P('ep'), may hold values from -0.125 to 0.125
- routed_down_weight: bfloat16 [32, 512, 2048], P('ep'), may hold values from -0.25 to 0.25
- common_gate_weight: bfloat16 [2048, 512], replicated, may hold values from -0.125 to 0.125
- common_up_weight: bfloat16 [2048, 512], replicated, may hold values from -0.125 to 0.125
- common_down_weight: bfloat16 [512, 2048], replicated, may hold values from -0.25 to 0.25
Outputs:
- hidden_out: bfloat16 [768, 2048], P(('grp', 'ep'))
- next_state: float32 [768, 16, 4096], P(('grp', 'ep'))
The draws below stay inside these ranges and needn't reach their ends.
Inputs may be any that keep to these rules, and one draw needn't show every extreme that they name: `routes`: the 4 entries of a row differ. In each aligned block of 24 rows (the tokens of one index of ep) no expert is named by more than 4 rows, a bound that some block reaches.
All inputs are finite; a program needn't handle non-finite values.
Results may differ from the reference program's by a relative error of at most 0.013.
Values may be sent and summed in bfloat16 or wider, within the bound.
A program may use at most 128 MiB of HBM per device.

```python
import math
import jax
import jax.numpy as jnp
import numpy as np
from jax import lax

D = 2048
HEAD_COUNT = 16
HEAD_SIZE = 64
MIXER_WIDTH = 1024
EFF = 512
SFF = 512
EXPERTS = 32
TOPK = 4
CAP = 4
SEQ_DEV = 24
TOKENS = 768
N_EP = 32


def block_levels(key, shape, shards, least, high):
    level, own = 1.0, jax.random.fold_in(key, 6)
    for position, blocks in shards:
        heights = jnp.exp(jax.random.uniform(jax.random.fold_in(own, position), (blocks,), jnp.float32, least / len(shards), high / len(shards)))
        level = level * jnp.repeat(heights, shape[position] // blocks).reshape([-1 if axis == position else 1 for axis in range(len(shape))])
    return level


def routed_block(key, own, number, rows, amount, top, reach, skew):
    sequence = jax.random.permutation(key, amount)
    heavy_load, common = shares(amount, rows * top, reach, skew, True), shares(amount, rows * top, reach, skew, False)
    places = jnp.arange(amount)

    def named(tallies, turn):
        used = int((tallies > 0).sum())
        fixed = max(1, used // 4)
        passed = fixed + (places - fixed + turn * (used - fixed)) % max(1, amount - fixed)
        return jnp.zeros((amount,), jnp.int32).at[sequence[jnp.where(places < fixed, places, passed)]].set(jnp.asarray(tallies, jnp.int32))

    tallies = jnp.where(number % 4 == 0, named(heavy_load, number // 4), named(common, number - number // 4 - 1))
    mixed = jax.random.permutation(jax.random.fold_in(own, 3), amount)
    source_of, receiver = mixed[0:amount // 2 * 2:2], mixed[1:amount // 2 * 2:2]
    room = jnp.minimum(tallies[source_of] - 1, reach - tallies[receiver]) // 2
    room = jnp.where((source_of == sequence[0]) | (receiver == sequence[0]) | (tallies[receiver] == 0), 0, jnp.maximum(room, 0))
    passed = jax.random.randint(jax.random.fold_in(own, 4), (amount // 2,), 0, 1 << 20) % (room + 1)
    tallies = tallies.at[source_of].add(-passed).at[receiver].add(passed)
    members = jnp.searchsorted(jnp.cumsum(tallies), jnp.arange(rows * top), side="right").astype(jnp.int32)
    table = members.reshape(top, rows).T
    table = table[jax.random.permutation(jax.random.fold_in(own, 1), rows)]
    turn = jax.random.randint(jax.random.fold_in(own, 2), (rows, 1), 0, top)
    return jnp.take_along_axis(table, (jnp.arange(top)[None, :] + turn) % top, axis=1)


def shares(count, total, most, slope, full):
    loads = [(1 << 20) // math.isqrt(rank ** slope) + 1 for rank in range(1, count + 1)]
    largest = most if full else min(most, max(-(-total // count), total * loads[0] // sum(loads)))
    least = 1 if total - largest >= count - 1 else 0
    given, rest = [largest] + [least] * (count - 1), total - largest - least * (count - 1)
    while rest > 0:
        candidates = [i for i in range(1, count) if given[i] < largest] or [i for i in range(1, count) if given[i] < most]
        mass, remaining = sum([loads[i] for i in candidates]), rest
        for i in candidates:
            extra = min(most - given[i], max(1, remaining * loads[i] // mass), rest)
            given[i] = given[i] + extra
            rest = rest - extra
    return np.array(given)


def scatter_about(own_key, dims, scale, most, shards=(), kind=jnp.bfloat16):
    level = block_levels(own_key, dims, shards, -0.22, 0.18) if shards else 1.0
    drawn = jax.random.normal(own_key, dims, jnp.float32) * scale * level
    return jnp.minimum(jnp.maximum(drawn, -most), most).astype(kind)


def setup_inputs(seed: int = 0, part: int = 0) -> dict:
    splits = jax.random.split(jax.random.key(seed), 24)
    part_keys = jax.random.split(jax.random.fold_in(splits[23], part), 24)
    residual_input = scatter_about(part_keys[0], (TOKENS, D), 1.0, 6.0, ((0, 32),))
    attention_norm_gain = jnp.clip(1.0 + 0.18 * jax.random.normal(splits[1], (D,), jnp.float32), 0.099609375, 1.8984375).astype(jnp.bfloat16)
    receptance_weight = scatter_about(splits[2], (D, MIXER_WIDTH), D ** -0.5, 0.125, ((1, 32),))
    key_weight = scatter_about(splits[3], (D, MIXER_WIDTH), D ** -0.5, 0.125, ((1, 32),))
    value_weight = scatter_about(splits[4], (D, MIXER_WIDTH), D ** -0.5, 0.125, ((1, 32),))
    decay_weight = scatter_about(splits[5], (D, MIXER_WIDTH), D ** -0.5, 0.125, ((1, 32),))
    correction_rate_weight = scatter_about(splits[6], (D, MIXER_WIDTH), D ** -0.5, 0.125, ((1, 32),))
    output_gate_weight = scatter_about(splits[7], (D, MIXER_WIDTH), D ** -0.5, 0.125, ((1, 32),))
    decay_offset = jnp.clip(jax.random.uniform(splits[8], (MIXER_WIDTH,), jnp.float32, -3.0, 1.0), -3.0, 1.0)
    correction_rate_offset = jnp.clip(jax.random.uniform(splits[9], (MIXER_WIDTH,), jnp.float32, -1.5, 1.5), -1.5, 1.5)
    self_term_weight = scatter_about(splits[10], (MIXER_WIDTH,), 0.15, 2.0, (), jnp.float32)
    head_read_gain = jnp.clip(1.0 + 0.18 * jax.random.normal(splits[11], (MIXER_WIDTH,), jnp.float32), 0.1, 1.9)
    previous_state = scatter_about(part_keys[12], (TOKENS, HEAD_COUNT, HEAD_SIZE * HEAD_SIZE), 0.3, 4.0, ((0, 32),), jnp.float32)
    attention_output_weight = scatter_about(splits[13], (MIXER_WIDTH, D), MIXER_WIDTH ** -0.5, 0.1875)
    feedforward_norm_gain = jnp.clip(1.0 + 0.18 * jax.random.normal(splits[14], (D,), jnp.float32), 0.099609375, 1.8984375).astype(jnp.bfloat16)
    routes_keys = jax.random.split(jax.random.fold_in(part_keys[15], 1), TOKENS // SEQ_DEV)
    routes_turns = jax.random.permutation(jax.random.fold_in(part_keys[15], 3), TOKENS // SEQ_DEV)
    routes = jax.vmap(lambda own, number: routed_block(jax.random.fold_in(part_keys[15], 2), own, number, SEQ_DEV, EXPERTS, TOPK, CAP, 2))(routes_keys, routes_turns).reshape((TOKENS, TOPK))
    routing_weight = jnp.clip(jax.random.uniform(part_keys[16], (TOKENS, TOPK), jnp.float32, 0.2, 1.0), 0.2, 1.0)
    routed_gate_weight = scatter_about(splits[17], (EXPERTS, D, EFF), D ** -0.5, 0.125, ((0, 32),))
    routed_up_weight = scatter_about(splits[18], (EXPERTS, D, EFF), D ** -0.5, 0.125, ((0, 32),))
    routed_down_weight = scatter_about(splits[19], (EXPERTS, EFF, D), EFF ** -0.5, 0.25, ((0, 32),))
    common_gate_weight = scatter_about(splits[20], (D, SFF), D ** -0.5, 0.125)
    common_up_weight = scatter_about(splits[21], (D, SFF), D ** -0.5, 0.125)
    common_down_weight = scatter_about(splits[22], (SFF, D), SFF ** -0.5, 0.25)
    return {"residual_input": residual_input, "attention_norm_gain": attention_norm_gain, "receptance_weight": receptance_weight, "key_weight": key_weight, "value_weight": value_weight, "decay_weight": decay_weight, "correction_rate_weight": correction_rate_weight, "output_gate_weight": output_gate_weight, "decay_offset": decay_offset, "correction_rate_offset": correction_rate_offset, "self_term_weight": self_term_weight, "head_read_gain": head_read_gain, "previous_state": previous_state, "attention_output_weight": attention_output_weight, "feedforward_norm_gain": feedforward_norm_gain, "routes": routes, "routing_weight": routing_weight, "routed_gate_weight": routed_gate_weight, "routed_up_weight": routed_up_weight, "routed_down_weight": routed_down_weight, "common_gate_weight": common_gate_weight, "common_up_weight": common_up_weight, "common_down_weight": common_down_weight}


def rms_norm(value_rows, gain):
    scale = lax.rsqrt(lax.optimization_barrier(jnp.mean(value_rows * value_rows, axis=-1, keepdims=True)) + 1e-06)
    return (value_rows * scale * gain.astype(jnp.float32)).astype(jnp.bfloat16)

def expert_mlp(rows, gate_w, up_w, down_w):
    gate = jnp.dot(rows, gate_w, preferred_element_type=jnp.float32)
    upward = jnp.dot(rows, up_w, preferred_element_type=jnp.float32)
    hidden = (jax.nn.silu(gate) * upward).astype(jnp.bfloat16)
    return jnp.dot(hidden, down_w, preferred_element_type=jnp.float32).astype(jnp.bfloat16)

def attention_mixer(receptance_rows, key_rows, value_rows, decay_logit, rate_logit, gate_logit, decay_offset, correction_rate_offset, self_term_weight, head_read_gain, head_state):
    tally_value = receptance_rows.shape[0]

    def heads(tensor):
        return tensor.astype(jnp.float32).reshape(tally_value, HEAD_COUNT, HEAD_SIZE)
    decay = jnp.exp(-jnp.exp(-jax.nn.softplus(-(decay_offset + decay_logit.astype(jnp.float32))) - 0.5))
    rate = jax.nn.sigmoid(correction_rate_offset + rate_logit.astype(jnp.float32))
    key_head = heads(key_rows)
    rate_head = heads(rate)
    receptance_head = heads(receptance_rows)
    head_value = heads(value_rows)
    unit_key = key_head * lax.rsqrt(1.0 + lax.optimization_barrier(jnp.sum(key_head * key_head, axis=-1, keepdims=True)))
    rate_scaled_key = key_head * rate_head
    removal = unit_key * rate_head
    matrix = head_state.reshape(tally_value, HEAD_COUNT, HEAD_SIZE, HEAD_SIZE)
    recalled = jnp.einsum('nhvk,nhk->nhv', matrix, unit_key, precision=lax.Precision.HIGHEST)
    matrix = matrix * heads(decay)[:, :, None, :] - recalled[..., None] * removal[:, :, None, :] + head_value[..., None] * rate_scaled_key[:, :, None, :]
    read = jnp.einsum('nhvk,nhk->nhv', matrix, receptance_head, precision=lax.Precision.HIGHEST)
    centered = read - lax.optimization_barrier(jnp.mean(read, axis=-1, keepdims=True))
    variance = lax.optimization_barrier(jnp.mean(centered * centered, axis=-1, keepdims=True))
    normed_head_read = centered * lax.rsqrt(variance + 0.00064) * head_read_gain.reshape(HEAD_COUNT, HEAD_SIZE)
    self_term = lax.optimization_barrier(jnp.sum(receptance_head * rate_scaled_key * self_term_weight.reshape(HEAD_COUNT, HEAD_SIZE), axis=-1, keepdims=True)) * head_value
    normed_mixer_input = (normed_head_read + self_term).reshape(tally_value, HEAD_COUNT * HEAD_SIZE) * jax.nn.sigmoid(gate_logit.astype(jnp.float32))
    return (normed_mixer_input.astype(jnp.bfloat16), matrix.reshape(tally_value, HEAD_COUNT, HEAD_SIZE * HEAD_SIZE))

def routed_sum(normed_ffn, routes, routing_weight, routed_gate_weight, routed_up_weight, routed_down_weight):
    tokens = normed_ffn.shape[0]
    limit = N_EP * CAP
    slots = jnp.arange(limit, dtype=jnp.int32)

    def add_expert(expert_id, total):
        match = routes == expert_id
        hit = jnp.any(match, axis=1).astype(jnp.int32)
        weight = lax.optimization_barrier(jnp.sum(jnp.where(match, routing_weight, 0.0), axis=1))
        rank = jnp.cumsum(hit) - hit
        select = (rank[None, :] == slots[:, None]) & (hit[None, :] == 1)
        rows = jnp.dot(select.astype(jnp.bfloat16), normed_ffn, preferred_element_type=jnp.float32).astype(jnp.bfloat16)
        output = expert_mlp(rows, routed_gate_weight[expert_id], routed_up_weight[expert_id], routed_down_weight[expert_id])
        spread = select.astype(jnp.float32).T * weight[:, None]
        return total + jnp.dot(spread, output.astype(jnp.float32), precision=lax.Precision.HIGHEST)
    return lax.fori_loop(0, EXPERTS, add_expert, jnp.zeros((tokens, normed_ffn.shape[1]), jnp.float32))

def reference(residual_input, attention_norm_gain, receptance_weight, key_weight, value_weight, decay_weight, correction_rate_weight, output_gate_weight, decay_offset, correction_rate_offset, self_term_weight, head_read_gain, previous_state, attention_output_weight, feedforward_norm_gain, routes, routing_weight, routed_gate_weight, routed_up_weight, routed_down_weight, common_gate_weight, common_up_weight, common_down_weight):
    normed = rms_norm(residual_input.astype(jnp.float32), attention_norm_gain)

    def apply_projection(weight):
        return jnp.dot(normed, weight, preferred_element_type=jnp.float32).astype(jnp.bfloat16)
    normed_mixer_input, next_state = attention_mixer(apply_projection(receptance_weight), apply_projection(key_weight), apply_projection(value_weight), apply_projection(decay_weight), apply_projection(correction_rate_weight), apply_projection(output_gate_weight), decay_offset, correction_rate_offset, self_term_weight, head_read_gain, previous_state)
    attended = jnp.dot(normed_mixer_input, attention_output_weight, preferred_element_type=jnp.float32).astype(jnp.bfloat16)
    middle = residual_input.astype(jnp.float32) + attended.astype(jnp.float32)
    normed_ffn = rms_norm(middle, feedforward_norm_gain)
    shared = expert_mlp(normed_ffn, common_gate_weight, common_up_weight, common_down_weight)
    routed = routed_sum(normed_ffn, routes, routing_weight, routed_gate_weight, routed_up_weight, routed_down_weight)
    hidden_out = (middle + shared.astype(jnp.float32) + routed).astype(jnp.bfloat16)
    return (hidden_out, next_state)
```

```python
import functools
import math

import jax
import jax.numpy as jnp
from jax import lax
from jax.experimental import pallas as pl
from jax.experimental.pallas import tpu as pltpu
from jax.sharding import PartitionSpec as P

HEAD_COUNT = 16
HEAD_SIZE = 64
CAP = 4
ROLES = 6
LANES = 128
F32 = jnp.float32
BF16 = jnp.bfloat16


def rms_norm(value_rows, gain):
    scale = lax.rsqrt(jnp.mean(value_rows * value_rows, axis=-1, keepdims=True) + 1e-06)
    return (value_rows * scale * gain.astype(F32)).astype(BF16)


def expert_mlp(rows, gate_w, up_w, down_w):
    gate = jnp.dot(rows, gate_w, preferred_element_type=F32)
    upward = jnp.dot(rows, up_w, preferred_element_type=F32)
    hidden = (jax.nn.silu(gate) * upward).astype(BF16)
    return jnp.dot(hidden, down_w, preferred_element_type=F32).astype(BF16)


def split(value):
    high = value.astype(BF16)
    return high, (value - high.astype(F32)).astype(BF16)


def dot(a, b):
    return jnp.dot(a, b, preferred_element_type=F32)


PLANE = 8
CORES = 2
COLUMNS = PLANE // CORES


def remote(source, target, device, send_sem, recv_sem):
    return pltpu.make_async_remote_copy(
        src_ref=source, dst_ref=target, send_sem=send_sem, recv_sem=recv_sem,
        device_id={"ep": device}, device_id_type=pl.DeviceIdType.MESH,
    )


def route_tables(routes, weights, me, tokens, select_out, coef_out):
    everyone = routes.shape[1]
    slots = select_out.shape[1]
    contract = (((1,), (1,)), ((), ()))
    mine = lax.broadcasted_iota(jnp.int32, (tokens, everyone), 1) - me * tokens
    pick = (mine == lax.broadcasted_iota(jnp.int32, (tokens, everyone), 0)).astype(F32).astype(BF16)

    def own(table):
        return lax.dot_general(pick, table, contract, preferred_element_type=F32)

    named = own(routes.astype(F32).astype(BF16))
    weight_high, weight_low = split(weights)
    own_high, own_low = own(weight_high), own(weight_low)
    lane = lax.broadcasted_iota(jnp.int32, (tokens, slots), 1)
    expert = (lane // CAP).astype(F32)
    hit = jnp.zeros((tokens, slots), F32)
    high, low = hit, hit
    for entry in range(routes.shape[0]):
        match = (named[:, entry : entry + 1] == expert).astype(F32)
        hit = hit + match
        high = high + match * own_high[:, entry : entry + 1]
        low = low + match * own_low[:, entry : entry + 1]
    later = lax.broadcasted_iota(jnp.int32, (tokens, tokens), 0)
    earlier = lax.broadcasted_iota(jnp.int32, (tokens, tokens), 1)
    before = (earlier < later).astype(F32).astype(BF16)
    rank = dot(before, hit.astype(BF16))
    chosen = hit * (rank == (lane % CAP).astype(F32)).astype(F32)
    select_out[...] = chosen
    coef_out[:tokens] = (chosen * high).astype(BF16)
    coef_out[tokens:] = (chosen * low).astype(BF16)


def place_matrix(piece, rows, width):
    lane = lax.broadcasted_iota(jnp.int32, (1, ROLES * LANES), 1)
    inner = lane % HEAD_SIZE - piece * CORES * width
    core = inner // width
    row = (core * ROLES + lane // LANES) * width + inner - core * width
    row = jnp.where((inner >= 0) & (inner < CORES * width), row, -1)
    here = lax.broadcasted_iota(jnp.int32, (rows, ROLES * LANES), 0)
    return (here == row).astype(F32).astype(BF16)


def gather_matrix(first, columns):
    value = first + lax.broadcasted_iota(jnp.int32, (columns, LANES), 0) // HEAD_SIZE
    lane = lax.broadcasted_iota(jnp.int32, (columns, LANES), 1) % HEAD_SIZE
    return (value == lane).astype(F32).astype(BF16)


def spread_matrix(first, columns):
    value = first + lax.broadcasted_iota(jnp.int32, (LANES, columns), 1) // HEAD_SIZE
    row = lax.broadcasted_iota(jnp.int32, (LANES, columns), 0) % HEAD_SIZE
    return (value == row).astype(F32).astype(BF16)


def gain_row(gain):
    rows = gain.astype(F32)
    return jnp.concatenate([rows[i : i + 1] for i in range(rows.shape[0])], axis=1)


PARTS = 4


def layer_kernel(
    depth,
    resid_hbm, gain_hbm, w0, w1, w2, w3, w4, w5, routes_hbm, rweight_hbm,
    const0, const1, const2, const3, state_hbm, out_w_hbm, ffn_gain_hbm, g0, g1, g2, g3, g4, g5,
    hidden_out, recalled_out, value_out, decay_out, removal_out, scaled_out,
    resid, gain, weight, routes, rweight, held, cols, land,
    raw, consts, state, out_w, ffn_gain, b0, b1, b2, b3, b4, b5,
    place, role_ref, unit_ref, query_ref, mixed_ref, select_ref, coef_ref,
    middle_ref, normed_ref, out_rows, served, output, returned,
    load_sem, weight_sem, state_sem, big_sem,
    z_send, z_recv, near_send, near_recv, half_send, half_recv, mate_send, mate_recv,
    out_send, out_recv, go_send, go_recv, back_send, back_recv,
):
    total = depth * PLANE
    chips = depth * COLUMNS
    tokens, model = resid_hbm.shape
    cut = model // 2
    me = lax.axis_index("ep")
    core = lax.rem(me, CORES)
    chip = me // CORES
    column = lax.rem(chip, COLUMNS)
    level = chip // COLUMNS
    x = lax.rem(column, 2)
    y = column // 2
    mate = me + 1 - 2 * core
    column_x = column + 1 - 2 * x
    column_y = column + 2 - 4 * y
    far = COLUMNS - 1 - column
    pieces = land.shape[1]
    rows_all = tokens * HEAD_COUNT

    def device(of_level, of_column):
        return (of_level * COLUMNS + of_column) * CORES + core

    along_x, along_y = device(level, column_x), device(level, column_y)

    barrier = pltpu.get_barrier_semaphore()

    def greet(number, carry):
        peer = lax.rem(me + number, total)
        pl.semaphore_signal(barrier, inc=1, device_id={"ep": peer}, device_id_type=pl.DeviceIdType.MESH)
        return carry

    lax.fori_loop(1, total, greet, 0)

    loads = [
        pltpu.make_async_copy(source, target, load_sem.at[i])
        for i, (source, target) in enumerate(
            (
                (resid_hbm, resid), (gain_hbm, gain), (routes_hbm, routes), (rweight_hbm, rweight),
                (const0, raw.at[0]), (const1, raw.at[1]), (const2, raw.at[2]), (const3, raw.at[3]),
                (ffn_gain_hbm, ffn_gain),
            )
        )
    ]
    for load in loads:
        load.start()
    weight_loads = [
        pltpu.make_async_copy(source, weight.at[core, i], weight_sem.at[i])
        for i, source in enumerate((w0, w1, w2, w3, w4, w5))
    ]
    for load in weight_loads:
        load.start()
    span = state.shape[2] // PARTS
    state_loads = [
        pltpu.make_async_copy(
            state_hbm.at[:, :, pl.ds(i * span, span)], state.at[:, :, pl.ds(i * span, span)], state_sem.at[i]
        )
        for i in range(PARTS)
    ]
    big_loads = [
        pltpu.make_async_copy(source, target, big_sem.at[i])
        for i, (source, target) in enumerate(
            ((out_w_hbm, out_w), (g0, b0), (g1, b1), (g2, b2), (g3, b3), (g4, b4), (g5, b5))
        )
    ]

    loads[0].wait()
    loads[1].wait()
    held[column, level] = rms_norm(resid[...].astype(F32), gain_row(gain[...]))
    for load in weight_loads:
        load.wait()
    for load in state_loads + big_loads:
        load.start()

    pl.semaphore_wait(barrier, total - 1)

    nearer = jnp.minimum(level, depth - 1 - level)

    def nearest(k):
        step = (k + 1) // 2 if k % 2 else -(k // 2)
        beyond = jnp.where(2 * level < depth - 1, k - nearer, nearer - k)
        return level + jnp.where(k <= 2 * nearer, step, beyond)

    order = [level] + [nearest(k) for k in range(1, depth)]

    def along_z(to, source, slot):
        return remote(held.at[column, slot], held.at[column, slot], device(to, column), z_send.at[to], z_recv.at[source])

    for to in order[1:]:
        along_z(to, level, level).start()

    sent = []

    def forward(slot):
        block = held.at[column, slot]
        for axis, target in ((0, along_y), (1, along_x)):
            copy = remote(block, block, target, near_send.at[axis, slot], near_recv.at[axis, slot])
            copy.start()
            sent.append(copy)

    def relay(slot):
        for axis, (of_column, target, part) in enumerate(
            ((column_y, along_x, slice(0, cut)), (column_x, along_y, slice(cut, model)))
        ):
            block = held.at[of_column, slot]
            remote(block, block, along_y, near_send.at[axis, slot], near_recv.at[axis, slot]).wait_recv()
            half = block.at[:, part]
            copy = remote(half, half, target, half_send.at[axis, slot], half_recv.at[axis, slot])
            copy.start()
            sent.append(copy)

    forward(level)
    swap = remote(weight.at[core], weight.at[core], mate, mate_send, mate_recv)
    swap.start()
    for load in loads[2:]:
        load.wait()
    route_tables(routes[...], rweight[...], me, tokens, select_ref, coef_ref)
    for number in range(4):
        pair = raw[number]
        turned = pltpu.roll(pair, HEAD_SIZE, 1)
        first = lax.broadcasted_iota(jnp.int32, pair.shape, 1) < HEAD_SIZE
        count = pair.shape[0]
        consts[number, pl.ds(0, count, stride=2), :] = jnp.where(first, pair, turned)
        consts[number, pl.ds(1, count, stride=2), :] = jnp.where(first, turned, pair)
    for piece in range(pieces):
        place[piece] = place_matrix(piece, place.shape[1], weight.shape[2])

    for before, slot in zip(order, order[1:]):
        along_z(slot, slot, slot).wait_recv()
        forward(slot)
        relay(before)
    swap.wait_recv()

    def compute(of_column):
        rows = held[of_column].astype(F32).reshape(depth * tokens, model).astype(BF16)
        both = weight[...]
        width = both.shape[2]
        if width % 16:
            both = both.astype(F32)
        both = both.reshape(CORES * ROLES * width, model).astype(BF16)
        result = lax.dot_general(rows, both, (((1,), (1,)), ((), ())), preferred_element_type=F32)
        cols[of_column] = result.reshape(depth, tokens, result.shape[-1]).astype(BF16)

    def handed(of_level, of_column):
        to_chip = of_level * COLUMNS + of_column
        number = lax.rem(to_chip - chip + chips, chips)
        return remote(
            cols.at[of_column, of_level], land.at[chip // pieces, lax.rem(chip, pieces)], to_chip * CORES + core,
            out_send.at[number], out_recv.at[number],
        )

    def give(of_column):
        for to in order:
            if of_column is column and to is level:
                land[chip // pieces, lax.rem(chip, pieces)] = cols[column, level]
            else:
                handed(to, of_column).start()

    compute(column)
    relay(order[-1])
    give(column)
    compute(column_y)
    give(column_y)
    compute(column_x)
    give(column_x)
    for slot in order:
        for axis, part in ((0, slice(0, cut)), (1, slice(cut, model))):
            half = held.at[far, slot].at[:, part]
            remote(half, half, along_x, half_send.at[axis, slot], half_recv.at[axis, slot]).wait_recv()
    compute(far)
    give(far)

    def finish(number, carry):
        to_chip = lax.rem(chip + number, chips)
        copy = remote(
            cols.at[0, 0], land.at[0, 0], to_chip * CORES + core, out_send.at[number], out_recv.at[number]
        )
        copy.wait_recv()
        copy.wait_send()
        return carry

    lax.fori_loop(1, chips, finish, 0)

    spread_out = jnp.zeros((rows_all, ROLES * LANES), F32)
    for piece in range(pieces):
        rows = land[:, piece].astype(F32).reshape(rows_all, land.shape[3]).astype(BF16)
        spread_out = spread_out + dot(rows, place[piece])
    for head in range(HEAD_COUNT):
        for number in range(ROLES):
            part = spread_out[head * tokens : (head + 1) * tokens, number * LANES : (number + 1) * LANES]
            role_ref[number, pl.ds(head, tokens, stride=HEAD_COUNT), :] = part

    def const(number):
        one = consts[number]
        return jnp.concatenate([one] * tokens, axis=0)

    half_lanes = HEAD_SIZE / LANES

    def head_sum(value):
        return jnp.sum(value, axis=-1, keepdims=True) * half_lanes

    receptance, keys, values = role_ref[0], role_ref[1], role_ref[2]
    decay = jnp.exp(-math.exp(-0.5) * jax.nn.sigmoid(const(0) + role_ref[3]))
    rate = jax.nn.sigmoid(const(1) + role_ref[4])
    unit_key = keys * lax.rsqrt(1.0 + head_sum(keys * keys))
    scaled_key = keys * rate
    removal = unit_key * rate
    self_sum = head_sum(receptance * scaled_key * const(2))
    removed = head_sum(removal * receptance)
    added = head_sum(scaled_key * receptance)
    unit_ref[...] = unit_key
    query_ref[...] = decay * receptance
    value_out[...] = values
    decay_out[...] = decay
    removal_out[...] = removal
    scaled_out[...] = scaled_key

    recalled = jnp.zeros((rows_all, LANES), F32)
    kept = jnp.zeros((rows_all, LANES), F32)
    for part in range(PARTS):
        state_loads[part].wait()
        pick = gather_matrix(part * span // HEAD_SIZE, span)
        block = state[:, :, part * span : (part + 1) * span].reshape(rows_all, span)
        wide_key = jnp.concatenate([unit_ref[...]] * (span // LANES), axis=1)
        recalled = recalled + dot((block * wide_key).astype(BF16), pick)
        wide_query = jnp.concatenate([query_ref[...]] * (span // LANES), axis=1)
        kept = kept + dot((block * wide_query).astype(BF16), pick)
    recalled_out[...] = recalled
    values = role_ref[2]
    read = kept - recalled * removed + values * added
    centered = read - head_sum(read) * (1.0 / HEAD_SIZE)
    variance = head_sum(centered * centered) * (1.0 / HEAD_SIZE)
    normal = centered * lax.rsqrt(variance + 0.00064) * const(3)
    mixed_ref[...] = (normal + self_sum * values) * jax.nn.sigmoid(role_ref[5])

    lane = lax.broadcasted_iota(jnp.int32, (tokens, LANES), 1)
    per = LANES // HEAD_SIZE
    parts = []
    for first in range(0, HEAD_COUNT, per):
        part = mixed_ref[pl.ds(first, tokens, stride=HEAD_COUNT), :]
        for other in range(1, per):
            rest = mixed_ref[pl.ds(first + other, tokens, stride=HEAD_COUNT), :]
            part = jnp.where(lane < other * HEAD_SIZE, part, rest)
        parts.append(part.astype(BF16))
    mixed = jnp.concatenate(parts, axis=1)
    big_loads[0].wait()
    attended = dot(mixed, out_w[...]).astype(BF16).astype(F32)
    middle = resid[...].astype(F32) + attended
    middle_ref[...] = middle
    normed = rms_norm(middle, gain_row(ffn_gain[...]))
    normed_ref[...] = normed
    picked = lax.dot_general(
        select_ref[...].astype(BF16), normed, (((0,), (0,)), ((), ())), preferred_element_type=F32
    )
    out_rows[...] = picked.reshape(out_rows.shape).astype(BF16)

    def go(number):
        to = lax.rem(me + number, total)
        return remote(out_rows.at[to], served.at[me], to, go_send.at[number], go_recv.at[number])

    def back(to):
        number = lax.rem(to - me + total, total)
        return remote(output.at[to], returned.at[me], to, back_send.at[number], back_recv.at[number])

    def launch(number, carry):
        go(number).start()
        return carry

    lax.fori_loop(1, total, launch, 0)
    served[me] = out_rows[me]
    for load in big_loads[1:4]:
        load.wait()
    shared = expert_mlp(normed_ref[...], b0[...], b1[...], b2[...])
    middle_ref[...] = middle_ref[...] + shared.astype(F32)
    for load in big_loads[4:]:
        load.wait()

    for d in range(depth):
        first = lax.rem(level + depth - d, depth) * PLANE

        def arrive(i, carry):
            source = first + i

            @pl.when(source != me)
            def _():
                go(lax.rem(me - source + total, total)).wait_recv()

            return carry

        lax.fori_loop(0, PLANE, arrive, 0)
        rows = served[pl.ds(first, PLANE)].reshape(PLANE * CAP, model)
        result = expert_mlp(rows, b3[...], b4[...], b5[...])
        output[pl.ds(first, PLANE)] = result.reshape(PLANE, CAP, model)

        def give_back(i, carry):
            source = first + i

            @pl.when(source != me)
            def _():
                back(source).start()

            return carry

        lax.fori_loop(0, PLANE, give_back, 0)
    returned[me] = output[me]

    def ended(number, carry):
        go(number).wait_send()
        copy = back(lax.rem(me + number, total))
        copy.wait_recv()
        copy.wait_send()
        return carry

    lax.fori_loop(1, total, ended, 0)
    routed = dot(coef_ref[...], returned[...].reshape(total * CAP, model))
    hidden_out[...] = (middle_ref[...] + (routed[:tokens] + routed[tokens:])).astype(BF16)

    for to in order[1:]:
        along_z(to, level, level).wait_send()
    for copy in sent:
        copy.wait_send()
    swap.wait_send()


def layer(resid, gain, weights, routes, routing_weight, consts, state, out_w, ffn_gain, experts, ep_size):
    depth = ep_size // PLANE
    chips = ep_size // CORES
    pieces = chips // HEAD_COUNT
    tokens, model = resid.shape
    weights = [w.T for w in weights]
    width = weights[0].shape[0]
    wide = CORES * ROLES * width
    rows_all = tokens * HEAD_COUNT
    routes, routing_weight = routes.T, routing_weight.T
    gain = gain.reshape(model // LANES, LANES)
    ffn_gain = ffn_gain.reshape(model // LANES, LANES)
    consts = [c.reshape(-1, LANES) for c in consts]
    slots = ep_size * CAP
    dma = pltpu.SemaphoreType.DMA
    hbm = pl.BlockSpec(memory_space=pltpu.HBM)
    vmem = pl.BlockSpec(memory_space=pltpu.VMEM)
    operands = (resid, gain, *weights, routes, routing_weight, *consts, state, out_w, ffn_gain, *experts)
    operands = [pltpu.with_memory_space_constraint(a, pltpu.HBM) for a in operands]
    lanes = jax.ShapeDtypeStruct((rows_all, LANES), F32)
    return pl.pallas_call(
        functools.partial(layer_kernel, depth),
        out_shape=(jax.ShapeDtypeStruct((tokens, model), BF16),) + (lanes,) * 5,
        in_specs=[hbm] * len(operands),
        out_specs=(vmem,) * 6,
        scratch_shapes=[
            pltpu.VMEM((tokens, model), BF16),
            pltpu.VMEM(gain.shape, BF16),
            pltpu.VMEM((CORES, ROLES, width, model), BF16),
            pltpu.VMEM(routes.shape, jnp.int32),
            pltpu.VMEM(routes.shape, F32),
            pltpu.VMEM((COLUMNS, depth, tokens, model), BF16),
            pltpu.VMEM((COLUMNS, depth, tokens, wide), BF16),
            pltpu.VMEM((HEAD_COUNT, pieces, tokens, wide), BF16),
            pltpu.VMEM((4,) + consts[0].shape, F32),
            pltpu.VMEM((4, HEAD_COUNT, LANES), F32),
            pltpu.VMEM(state.shape, F32),
            pltpu.VMEM(out_w.shape, BF16),
            pltpu.VMEM(gain.shape, BF16),
        ]
        + [pltpu.VMEM(w.shape, BF16) for w in experts]
        + [
            pltpu.VMEM((pieces, wide, ROLES * LANES), BF16),
            pltpu.VMEM((ROLES, rows_all, LANES), F32),
            pltpu.VMEM((rows_all, LANES), F32),
            pltpu.VMEM((rows_all, LANES), F32),
            pltpu.VMEM((rows_all, LANES), F32),
            pltpu.VMEM((tokens, slots), F32),
            pltpu.VMEM((2 * tokens, slots), BF16),
            pltpu.VMEM((tokens, model), F32),
            pltpu.VMEM((tokens, model), BF16),
        ]
        + [pltpu.VMEM((ep_size, CAP, model), BF16)] * 4
        + [
            dma((9,)), dma((ROLES,)), dma((PARTS,)), dma((7,)),
            dma((depth,)), dma((depth,)),
            dma((2, depth)), dma((2, depth)),
            dma((2, depth)), dma((2, depth)),
            dma, dma,
            dma((chips,)), dma((chips,)),
        ]
        + [dma((ep_size,))] * 4,
        compiler_params=pltpu.CompilerParams(
            has_side_effects=True, collective_id=0, vmem_limit_bytes=52 * 1024 * 1024
        ),
        cost_estimate=pl.CostEstimate(flops=30_000_000_000, bytes_accessed=100_000_000, transcendentals=0),
    )(*operands)


def update_kernel(
    state, recalled, value, decay, removal, scaled, hidden, next_hbm, hidden_hbm, held, next_sem, hidden_sem
):
    copy = pltpu.make_async_copy(hidden, hidden_hbm, hidden_sem)
    copy.start()
    group, heads, columns = state.shape
    rows_all = group * heads
    span = columns // PARTS
    step = 4 * HEAD_SIZE
    lane = lax.broadcasted_iota(jnp.int32, (rows_all, LANES), 1)
    high, low = split(recalled[...])
    both = jnp.where(lane < HEAD_SIZE, high.astype(F32), low.astype(F32)).astype(BF16)
    alone = jnp.where(lane < HEAD_SIZE, value[...], 0.0).astype(BF16)
    stacked = jnp.concatenate([both, alone], axis=0)

    def twice(ref):
        return jnp.concatenate([ref[...]] * (step // LANES), axis=1)

    copies = []
    for part in range(PARTS):
        for first in range(part * span, (part + 1) * span, step):
            spread = dot(stacked, spread_matrix(first // HEAD_SIZE, step))
            block = state[:, :, first : first + step].reshape(rows_all, step)
            new = block * twice(decay) - spread[:rows_all] * twice(removal) + spread[rows_all:] * twice(scaled)
            held[:, :, first : first + step] = new.reshape(group, heads, step)
        here = pl.ds(part * span, span)
        out = pltpu.make_async_copy(held.at[:, :, here], next_hbm.at[:, :, here], next_sem.at[part])
        out.start()
        copies.append(out)
    for out in copies:
        out.wait()
    copy.wait()


def update(state, recalled, value, decay, removal, scaled, hidden):
    vmem = pl.BlockSpec(memory_space=pltpu.VMEM)
    hbm = pl.BlockSpec(memory_space=pltpu.HBM)
    dma = pltpu.SemaphoreType.DMA
    return pl.pallas_call(
        update_kernel,
        out_shape=(
            jax.ShapeDtypeStruct(state.shape, F32),
            jax.ShapeDtypeStruct(hidden.shape, BF16),
        ),
        in_specs=[vmem] * 7,
        out_specs=(hbm, hbm),
        scratch_shapes=[pltpu.VMEM(state.shape, F32), dma((PARTS,)), dma],
        compiler_params=pltpu.CompilerParams(vmem_limit_bytes=20 * 1024 * 1024),
        cost_estimate=pl.CostEstimate(flops=1_000_000_000, bytes_accessed=20_000_000, transcendentals=0),
    )(state, recalled, value, decay, removal, scaled, hidden)


def per_device(
    residual_input,
    attention_norm_gain,
    receptance_weight,
    key_weight,
    value_weight,
    decay_weight,
    correction_rate_weight,
    output_gate_weight,
    decay_offset,
    correction_rate_offset,
    self_term_weight,
    head_read_gain,
    previous_state,
    attention_output_weight,
    feedforward_norm_gain,
    routes,
    routing_weight,
    routed_gate_weight,
    routed_up_weight,
    routed_down_weight,
    common_gate_weight,
    common_up_weight,
    common_down_weight,
):
    ep_size = lax.axis_size("ep")
    hidden, recalled, value, decay, removal, scaled = layer(
        residual_input,
        attention_norm_gain,
        (
            receptance_weight,
            key_weight,
            value_weight,
            decay_weight,
            correction_rate_weight,
            output_gate_weight,
        ),
        routes,
        routing_weight,
        (decay_offset, correction_rate_offset, self_term_weight, head_read_gain),
        previous_state,
        attention_output_weight,
        feedforward_norm_gain,
        (
            common_gate_weight,
            common_up_weight,
            common_down_weight,
            routed_gate_weight[0],
            routed_up_weight[0],
            routed_down_weight[0],
        ),
        ep_size,
    )
    next_state, hidden_out = update(previous_state, recalled, value, decay, removal, scaled, hidden)
    return (hidden_out, next_state)


def solution(mesh):
    return jax.shard_map(
        per_device,
        mesh=mesh,
        in_specs=(
            P(("grp", "ep"), None),
            P(),
            P(None, "ep"),
            P(None, "ep"),
            P(None, "ep"),
            P(None, "ep"),
            P(None, "ep"),
            P(None, "ep"),
            P(),
            P(),
            P(),
            P(),
            P(("grp", "ep"), None, None),
            P(),
            P(),
            P("grp", None),
            P("grp", None),
            P("ep", None, None),
            P("ep", None, None),
            P("ep", None, None),
            P(),
            P(),
            P(),
        ),
        out_specs=(P(("grp", "ep"), None), P(("grp", "ep"), None, None)),
        check_vma=False,
    )
```

```python
import functools
import math

import jax
import jax.numpy as jnp
from jax import lax
from jax.experimental import pallas as pl
from jax.experimental.pallas import tpu as pltpu
from jax.sharding import PartitionSpec as P

HEAD_COUNT = 16
HEAD_SIZE = 64
CAP = 4
ROLES = 6
LANES = 128
F32 = jnp.float32
BF16 = jnp.bfloat16


def rms_norm(value_rows, gain):
    scale = lax.rsqrt(jnp.mean(value_rows * value_rows, axis=-1, keepdims=True) + 1e-06)
    return (value_rows * scale * gain.astype(F32)).astype(BF16)


def expert_mlp(rows, gate_w, up_w, down_w):
    gate = jnp.dot(rows, gate_w, preferred_element_type=F32)
    upward = jnp.dot(rows, up_w, preferred_element_type=F32)
    hidden = (jax.nn.silu(gate) * upward).astype(BF16)
    return jnp.dot(hidden, down_w, preferred_element_type=F32).astype(BF16)


def split(value):
    high = value.astype(BF16)
    return high, (value - high.astype(F32)).astype(BF16)


def dot(a, b):
    return jnp.dot(a, b, preferred_element_type=F32)


PLANE = 8
CORES = 2
COLUMNS = PLANE // CORES


def remote(source, target, device, send_sem, recv_sem):
    return pltpu.make_async_remote_copy(
        src_ref=source, dst_ref=target, send_sem=send_sem, recv_sem=recv_sem,
        device_id={"ep": device}, device_id_type=pl.DeviceIdType.MESH,
    )


def route_tables(routes, weights, me, tokens, select_out, coef_out):
    everyone = routes.shape[1]
    slots = select_out.shape[1]
    contract = (((1,), (1,)), ((), ()))
    mine = lax.broadcasted_iota(jnp.int32, (tokens, everyone), 1) - me * tokens
    pick = (mine == lax.broadcasted_iota(jnp.int32, (tokens, everyone), 0)).astype(F32).astype(BF16)

    def own(table):
        return lax.dot_general(pick, table, contract, preferred_element_type=F32)

    named = own(routes.astype(F32).astype(BF16))
    weight_high, weight_low = split(weights)
    own_high, own_low = own(weight_high), own(weight_low)
    lane = lax.broadcasted_iota(jnp.int32, (tokens, slots), 1)
    expert = (lane // CAP).astype(F32)
    hit = jnp.zeros((tokens, slots), F32)
    high, low = hit, hit
    for entry in range(routes.shape[0]):
        match = (named[:, entry : entry + 1] == expert).astype(F32)
        hit = hit + match
        high = high + match * own_high[:, entry : entry + 1]
        low = low + match * own_low[:, entry : entry + 1]
    later = lax.broadcasted_iota(jnp.int32, (tokens, tokens), 0)
    earlier = lax.broadcasted_iota(jnp.int32, (tokens, tokens), 1)
    before = (earlier < later).astype(F32).astype(BF16)
    rank = dot(before, hit.astype(BF16))
    chosen = hit * (rank == (lane % CAP).astype(F32)).astype(F32)
    select_out[...] = chosen
    coef_out[:tokens] = (chosen * high).astype(BF16)
    coef_out[tokens:] = (chosen * low).astype(BF16)


def place_matrix(piece, rows, width):
    lane = lax.broadcasted_iota(jnp.int32, (1, ROLES * LANES), 1)
    inner = lane % HEAD_SIZE - piece * CORES * width
    core = inner // width
    row = (core * ROLES + lane // LANES) * width + inner - core * width
    row = jnp.where((inner >= 0) & (inner < CORES * width), row, -1)
    here = lax.broadcasted_iota(jnp.int32, (rows, ROLES * LANES), 0)
    return (here == row).astype(F32).astype(BF16)


def gather_matrix(first, columns):
    value = first + lax.broadcasted_iota(jnp.int32, (columns, LANES), 0) // HEAD_SIZE
    lane = lax.broadcasted_iota(jnp.int32, (columns, LANES), 1) % HEAD_SIZE
    return (value == lane).astype(F32).astype(BF16)


def spread_matrix(first, columns):
    value = first + lax.broadcasted_iota(jnp.int32, (LANES, columns), 1) // HEAD_SIZE
    row = lax.broadcasted_iota(jnp.int32, (LANES, columns), 0) % HEAD_SIZE
    return (value == row).astype(F32).astype(BF16)


def gain_row(gain):
    rows = gain.astype(F32)
    return jnp.concatenate([rows[i : i + 1] for i in range(rows.shape[0])], axis=1)


PARTS = 4
STORES = 8
UNITS = 2


def layer_kernel(
    depth,
    resid_hbm, gain_hbm, w0, w1, w2, w3, w4, w5, routes_hbm, rweight_hbm,
    const0, const1, const2, const3, state_hbm, out_w_hbm, ffn_gain_hbm, g0, g1, g2, g3, g4, g5,
    hidden_out, state,
    resid, gain, weight, routes, rweight, held, cols, land,
    raw, consts, out_w, ffn_gain, b0, b1, b2, b3, b4, b5,
    place, role_ref, unit_ref, query_ref, mixed_ref, recalled_ref, decay_ref, removal_ref, scaled_ref, select_ref, coef_ref,
    middle_ref, normed_ref, out_rows, served, output, returned,
    load_sem, weight_sem, state_sem, big_sem,
    z_send, z_recv, near_send, near_recv, half_send, half_recv, mate_send, mate_recv,
    out_send, out_recv, go_send, go_recv, back_send, back_recv,
):
    total = depth * PLANE
    chips = depth * COLUMNS
    tokens, model = resid_hbm.shape
    cut = model // UNITS
    me = lax.axis_index("ep")
    core = lax.rem(me, CORES)
    chip = me // CORES
    column = lax.rem(chip, COLUMNS)
    level = chip // COLUMNS
    x = lax.rem(column, 2)
    y = column // 2
    mate = me + 1 - 2 * core
    column_x = column + 1 - 2 * x
    column_y = column + 2 - 4 * y
    far = COLUMNS - 1 - column
    pieces = land.shape[1]
    rows_all = tokens * HEAD_COUNT

    def device(of_level, of_column):
        return (of_level * COLUMNS + of_column) * CORES + core

    along_x, along_y = device(level, column_x), device(level, column_y)

    barrier = pltpu.get_barrier_semaphore()

    loads = [
        pltpu.make_async_copy(source, target, load_sem.at[i])
        for i, (source, target) in enumerate(
            (
                (resid_hbm, resid), (gain_hbm, gain), (routes_hbm, routes), (rweight_hbm, rweight),
                (const0, raw.at[0]), (const1, raw.at[1]), (const2, raw.at[2]), (const3, raw.at[3]),
                (ffn_gain_hbm, ffn_gain),
            )
        )
    ]
    for load in loads[:2]:
        load.start()

    def greet(number, carry):
        peer = lax.rem(me + number, total)
        pl.semaphore_signal(barrier, inc=1, device_id={"ep": peer}, device_id_type=pl.DeviceIdType.MESH)
        return carry

    lax.fori_loop(1, total, greet, 0)

    for load in loads[2:]:
        load.start()
    weight_loads = [
        pltpu.make_async_copy(source, weight.at[core, i], weight_sem.at[i])
        for i, source in enumerate((w0, w1, w2, w3, w4, w5))
    ]
    for load in weight_loads:
        load.start()
    span = state.shape[2] // PARTS
    state_loads = [
        pltpu.make_async_copy(
            state_hbm.at[:, :, pl.ds(i * span, span)], state.at[:, :, pl.ds(i * span, span)], state_sem.at[i]
        )
        for i in range(PARTS)
    ]
    big_loads = [
        pltpu.make_async_copy(source, target, big_sem.at[i])
        for i, (source, target) in enumerate(
            ((out_w_hbm, out_w), (g0, b0), (g1, b1), (g2, b2), (g3, b3), (g4, b4), (g5, b5))
        )
    ]

    loads[0].wait()
    loads[1].wait()
    held[column, level] = rms_norm(resid[...].astype(F32), gain_row(gain[...]))
    pl.semaphore_wait(barrier, total - 1)

    nearer = jnp.minimum(level, depth - 1 - level)

    def nearest(k):
        step = (k + 1) // 2 if k % 2 else -(k // 2)
        beyond = jnp.where(2 * level < depth - 1, k - nearer, nearer - k)
        return level + jnp.where(k <= 2 * nearer, step, beyond)

    order = [level] + [nearest(k) for k in range(1, depth)]

    halves = [slice(i * cut, (i + 1) * cut) for i in range(UNITS)]
    turns = UNITS // 2

    def along_z(to, slot, half):
        block = held.at[column, slot].at[:, halves[half]]
        downward = jnp.where(to > level, 0, 1)
        return remote(
            block, block, device(to, column), z_send.at[downward, slot, half], z_recv.at[slot, half]
        )

    def each_way(act):
        for half in range(UNITS):
            for to in (level + 1, level - 1):

                @pl.when((to >= 0) & (to < depth))
                def _():
                    act(along_z(to, level, half))

    def onward(slot, half, act):
        to = jnp.where(slot > level, level - 1, level + 1)

        @pl.when((to >= 0) & (to < depth))
        def _():
            act(along_z(to, slot, half))

    each_way(lambda copy: copy.start())
    sent = []

    def near(axis, of_column, slot, half, target):
        block = held.at[of_column, slot].at[:, halves[half]]
        return remote(block, block, target, near_send.at[axis, slot, half], near_recv.at[axis, slot, half])

    def forward(slot, half):
        for axis, target in ((0, along_y), (1, along_x)):
            copy = near(axis, column, slot, half, target)
            copy.start()
            sent.append(copy)

    def relay(slot, turn):
        for axis, (of_column, target) in enumerate(((column_y, along_x), (column_x, along_y))):
            unit = axis * turns + turn
            near(axis, of_column, slot, unit, target).wait_recv()
            block = held.at[of_column, slot].at[:, halves[unit]]
            copy = remote(block, block, target, half_send.at[slot, unit], half_recv.at[slot, unit])
            copy.start()
            sent.append(copy)

    for half in range(UNITS):
        forward(level, half)
    for load in weight_loads:
        load.wait()
    for load in state_loads + big_loads:
        load.start()
    swap = remote(weight.at[core], weight.at[core], mate, mate_send, mate_recv)
    swap.start()
    for load in loads[2:]:
        load.wait()
    route_tables(routes[...], rweight[...], me, tokens, select_ref, coef_ref)
    for number in range(4):
        pair = raw[number]
        turned = pltpu.roll(pair, HEAD_SIZE, 1)
        first = lax.broadcasted_iota(jnp.int32, pair.shape, 1) < HEAD_SIZE
        count = pair.shape[0]
        consts[number, pl.ds(0, count, stride=2), :] = jnp.where(first, pair, turned)
        consts[number, pl.ds(1, count, stride=2), :] = jnp.where(first, turned, pair)
    for piece in range(pieces):
        place[piece] = place_matrix(piece, place.shape[1], weight.shape[2])

    for before, slot in zip(order, order[1:]):
        for half in range(UNITS):
            along_z(level, slot, half).wait_recv()
            onward(slot, half, lambda copy: copy.start())
            forward(slot, half)
            if half % 2:
                relay(before, half // 2)
    swap.wait_recv()

    def compute(of_column, slots):
        rows = jnp.concatenate([held[of_column, slot].astype(F32) for slot in slots], axis=0).astype(BF16)
        both = weight[...]
        width = both.shape[2]
        if width % 16:
            both = both.astype(F32)
        both = both.reshape(CORES * ROLES * width, model).astype(BF16)
        result = lax.dot_general(rows, both, (((1,), (1,)), ((), ())), preferred_element_type=F32)
        for i, slot in enumerate(slots):
            cols[of_column, slot] = result[i * tokens : (i + 1) * tokens].astype(BF16)

    def handed(of_level, of_column):
        to_chip = of_level * COLUMNS + of_column
        number = lax.rem(to_chip - chip + chips, chips)
        return remote(
            cols.at[of_column, of_level], land.at[chip // pieces, lax.rem(chip, pieces)], to_chip * CORES + core,
            out_send.at[number], out_recv.at[number],
        )

    def give(of_column, slots):
        for to in slots:
            if of_column is column and to is level:
                land[chip // pieces, lax.rem(chip, pieces)] = cols[column, level]
            else:
                handed(to, of_column).start()

    compute(column, order)
    give(column, order)
    for turn in range(turns):
        relay(order[-1], turn)
    for axis, of_column in ((0, column_y), (1, column_x)):
        for slot in order:
            for turn in range(turns):
                near(axis, of_column, slot, (1 - axis) * turns + turn, along_x).wait_recv()
        compute(of_column, order)
        give(of_column, order)
    for slots in (order[:-1], order[-1:]):
        for slot in slots:
            for unit in range(UNITS):
                block = held.at[far, slot].at[:, halves[unit]]
                remote(block, block, along_x, half_send.at[slot, unit], half_recv.at[slot, unit]).wait_recv()
        compute(far, slots)
        give(far, slots)

    def finish(number, carry):
        to_chip = lax.rem(chip + number, chips)
        copy = remote(
            cols.at[0, 0], land.at[0, 0], to_chip * CORES + core, out_send.at[number], out_recv.at[number]
        )
        copy.wait_recv()
        copy.wait_send()
        return carry

    lax.fori_loop(1, chips, finish, 0)

    spread_out = jnp.zeros((rows_all, ROLES * LANES), F32)
    for piece in range(pieces):
        rows = land[:, piece].astype(F32).reshape(rows_all, land.shape[3]).astype(BF16)
        spread_out = spread_out + dot(rows, place[piece])
    for head in range(HEAD_COUNT):
        for number in range(ROLES):
            part = spread_out[head * tokens : (head + 1) * tokens, number * LANES : (number + 1) * LANES]
            role_ref[number, pl.ds(head, tokens, stride=HEAD_COUNT), :] = part

    def const(number):
        one = consts[number]
        return jnp.concatenate([one] * tokens, axis=0)

    half_lanes = HEAD_SIZE / LANES

    def head_sum(value):
        return jnp.sum(value, axis=-1, keepdims=True) * half_lanes

    receptance, keys, values = role_ref[0], role_ref[1], role_ref[2]
    decay = jnp.exp(-math.exp(-0.5) * jax.nn.sigmoid(const(0) + role_ref[3]))
    rate = jax.nn.sigmoid(const(1) + role_ref[4])
    unit_key = keys * lax.rsqrt(1.0 + head_sum(keys * keys))
    scaled_key = keys * rate
    removal = unit_key * rate
    self_sum = head_sum(receptance * scaled_key * const(2))
    removed = head_sum(removal * receptance)
    added = head_sum(scaled_key * receptance)
    unit_ref[...] = unit_key
    query_ref[...] = decay * receptance
    decay_ref[...] = decay
    removal_ref[...] = removal
    scaled_ref[...] = scaled_key

    recalled = jnp.zeros((rows_all, LANES), F32)
    kept = jnp.zeros((rows_all, LANES), F32)
    for part in range(PARTS):
        state_loads[part].wait()
        pick = gather_matrix(part * span // HEAD_SIZE, span)
        block = state[:, :, part * span : (part + 1) * span].reshape(rows_all, span)
        wide_key = jnp.concatenate([unit_ref[...]] * (span // LANES), axis=1)
        recalled = recalled + dot((block * wide_key).astype(BF16), pick)
        wide_query = jnp.concatenate([query_ref[...]] * (span // LANES), axis=1)
        kept = kept + dot((block * wide_query).astype(BF16), pick)
    recalled_ref[...] = recalled
    values = role_ref[2]
    read = kept - recalled * removed + values * added
    centered = read - head_sum(read) * (1.0 / HEAD_SIZE)
    variance = head_sum(centered * centered) * (1.0 / HEAD_SIZE)
    normal = centered * lax.rsqrt(variance + 0.00064) * const(3)
    mixed_ref[...] = (normal + self_sum * values) * jax.nn.sigmoid(role_ref[5])

    lane = lax.broadcasted_iota(jnp.int32, (tokens, LANES), 1)
    per = LANES // HEAD_SIZE
    parts = []
    for first in range(0, HEAD_COUNT, per):
        part = mixed_ref[pl.ds(first, tokens, stride=HEAD_COUNT), :]
        for other in range(1, per):
            rest = mixed_ref[pl.ds(first + other, tokens, stride=HEAD_COUNT), :]
            part = jnp.where(lane < other * HEAD_SIZE, part, rest)
        parts.append(part.astype(BF16))
    mixed = jnp.concatenate(parts, axis=1)
    big_loads[0].wait()
    attended = dot(mixed, out_w[...]).astype(BF16).astype(F32)
    middle = resid[...].astype(F32) + attended
    middle_ref[...] = middle
    normed = rms_norm(middle, gain_row(ffn_gain[...]))
    normed_ref[...] = normed
    picked = lax.dot_general(
        select_ref[...].astype(BF16), normed, (((0,), (0,)), ((), ())), preferred_element_type=F32
    )
    out_rows[...] = picked.reshape(out_rows.shape).astype(BF16)

    def go(number):
        to = lax.rem(me + number, total)
        return remote(out_rows.at[to], served.at[me], to, go_send.at[number], go_recv.at[number])

    def back(to):
        number = lax.rem(to - me + total, total)
        return remote(output.at[to], returned.at[me], to, back_send.at[number], back_recv.at[number])

    place_in_plane = lax.rem(me, PLANE)

    def launch(of_level):
        def one(i, carry):
            to = of_level * PLANE + lax.rem(place_in_plane + i, PLANE)

            @pl.when(to != me)
            def _():
                go(lax.rem(to - me + total, total)).start()

            return carry

        lax.fori_loop(0, PLANE, one, 0)

    for of_level in order[::-1]:
        launch(of_level)
    served[me] = out_rows[me]
    for load in big_loads[1:4]:
        load.wait()
    shared = expert_mlp(normed_ref[...], b0[...], b1[...], b2[...])
    middle_ref[...] = middle_ref[...] + shared.astype(F32)
    for load in big_loads[4:]:
        load.wait()

    own_lane = lax.broadcasted_iota(jnp.int32, (rows_all, LANES), 1) < HEAD_SIZE
    high, low = split(recalled_ref[...])
    both = jnp.where(own_lane, high.astype(F32), low.astype(F32)).astype(BF16)
    alone = jnp.where(own_lane, role_ref[2], 0.0).astype(BF16)
    stacked = jnp.concatenate([both, alone], axis=0)
    step = 4 * HEAD_SIZE

    def twice(ref):
        return jnp.concatenate([ref[...]] * (step // LANES), axis=1)

    for first in range(0, state.shape[2], step):
        spread = dot(stacked, spread_matrix(first // HEAD_SIZE, step))
        block = state[:, :, first : first + step].reshape(rows_all, step)
        new = block * twice(decay_ref) - spread[:rows_all] * twice(removal_ref)
        new = new + spread[rows_all:] * twice(scaled_ref)
        state[:, :, first : first + step] = new.reshape(tokens, HEAD_COUNT, step)

    for of_level in order[::-1]:
        first = of_level * PLANE

        def arrive(i, carry):
            source = first + i

            @pl.when(source != me)
            def _():
                go(lax.rem(me - source + total, total)).wait_recv()

            return carry

        lax.fori_loop(0, PLANE, arrive, 0)
        rows = served[pl.ds(first, PLANE)].reshape(PLANE * CAP, model)
        result = expert_mlp(rows, b3[...], b4[...], b5[...])
        output[pl.ds(first, PLANE)] = result.reshape(PLANE, CAP, model)

        def give_back(i, carry):
            source = first + i

            @pl.when(source != me)
            def _():
                back(source).start()

            return carry

        lax.fori_loop(0, PLANE, give_back, 0)
    returned[me] = output[me]

    def ended(number, carry):
        go(number).wait_send()
        copy = back(lax.rem(me + number, total))
        copy.wait_recv()
        copy.wait_send()
        return carry

    lax.fori_loop(1, total, ended, 0)
    routed = dot(coef_ref[...], returned[...].reshape(total * CAP, model))
    hidden_out[...] = (middle_ref[...] + (routed[:tokens] + routed[tokens:])).astype(BF16)

    each_way(lambda copy: copy.wait_send())
    for slot in order[1:]:
        for half in range(UNITS):
            onward(slot, half, lambda copy: copy.wait_send())
    for copy in sent:
        copy.wait_send()
    swap.wait_send()


def layer(resid, gain, weights, routes, routing_weight, consts, state, out_w, ffn_gain, experts, ep_size):
    depth = ep_size // PLANE
    chips = ep_size // CORES
    pieces = chips // HEAD_COUNT
    tokens, model = resid.shape
    weights = [w.T for w in weights]
    width = weights[0].shape[0]
    wide = CORES * ROLES * width
    rows_all = tokens * HEAD_COUNT
    routes, routing_weight = routes.T, routing_weight.T
    gain = gain.reshape(model // LANES, LANES)
    ffn_gain = ffn_gain.reshape(model // LANES, LANES)
    consts = [c.reshape(-1, LANES) for c in consts]
    slots = ep_size * CAP
    dma = pltpu.SemaphoreType.DMA
    hbm = pl.BlockSpec(memory_space=pltpu.HBM)
    vmem = pl.BlockSpec(memory_space=pltpu.VMEM)
    operands = (resid, gain, *weights, routes, routing_weight, *consts, state, out_w, ffn_gain, *experts)
    operands = [pltpu.with_memory_space_constraint(a, pltpu.HBM) for a in operands]
    return pl.pallas_call(
        functools.partial(layer_kernel, depth),
        out_shape=(jax.ShapeDtypeStruct((tokens, model), BF16), jax.ShapeDtypeStruct(state.shape, F32)),
        in_specs=[hbm] * len(operands),
        out_specs=(vmem,) * 2,
        scratch_shapes=[
            pltpu.VMEM((tokens, model), BF16),
            pltpu.VMEM(gain.shape, BF16),
            pltpu.VMEM((CORES, ROLES, width, model), BF16),
            pltpu.VMEM(routes.shape, jnp.int32),
            pltpu.VMEM(routes.shape, F32),
            pltpu.VMEM((COLUMNS, depth, tokens, model), BF16),
            pltpu.VMEM((COLUMNS, depth, tokens, wide), BF16),
            pltpu.VMEM((HEAD_COUNT, pieces, tokens, wide), BF16),
            pltpu.VMEM((4,) + consts[0].shape, F32),
            pltpu.VMEM((4, HEAD_COUNT, LANES), F32),
            pltpu.VMEM(out_w.shape, BF16),
            pltpu.VMEM(gain.shape, BF16),
        ]
        + [pltpu.VMEM(w.shape, BF16) for w in experts]
        + [
            pltpu.VMEM((pieces, wide, ROLES * LANES), BF16),
            pltpu.VMEM((ROLES, rows_all, LANES), F32),
        ]
        + [pltpu.VMEM((rows_all, LANES), F32)] * 7
        + [
            pltpu.VMEM((tokens, slots), F32),
            pltpu.VMEM((2 * tokens, slots), BF16),
            pltpu.VMEM((tokens, model), F32),
            pltpu.VMEM((tokens, model), BF16),
        ]
        + [pltpu.VMEM((ep_size, CAP, model), BF16)] * 4
        + [
            dma((9,)), dma((ROLES,)), dma((PARTS,)), dma((7,)),
            dma((2, depth, UNITS)), dma((depth, UNITS)),
            dma((2, depth, UNITS)), dma((2, depth, UNITS)),
            dma((depth, UNITS)), dma((depth, UNITS)),
            dma, dma,
            dma((chips,)), dma((chips,)),
        ]
        + [dma((ep_size,))] * 4,
        compiler_params=pltpu.CompilerParams(
            has_side_effects=True, collective_id=0, vmem_limit_bytes=46 * 1024 * 1024
        ),
        cost_estimate=pl.CostEstimate(flops=30_000_000_000, bytes_accessed=100_000_000, transcendentals=0),
    )(*operands)


def store_kernel(state, hidden, next_hbm, hidden_hbm, next_sem, hidden_sem):
    parts = next_sem.shape[0]
    group = state.shape[0] // parts
    copies = [pltpu.make_async_copy(hidden, hidden_hbm, hidden_sem)]
    for part in range(parts):
        here = pl.ds(part * group, group)
        copies.append(pltpu.make_async_copy(state.at[here], next_hbm.at[here], next_sem.at[part]))
    for copy in copies:
        copy.start()
    for copy in copies:
        copy.wait()


def store(state, hidden):
    vmem = pl.BlockSpec(memory_space=pltpu.VMEM)
    hbm = pl.BlockSpec(memory_space=pltpu.HBM)
    dma = pltpu.SemaphoreType.DMA
    return pl.pallas_call(
        store_kernel,
        out_shape=(jax.ShapeDtypeStruct(state.shape, F32), jax.ShapeDtypeStruct(hidden.shape, BF16)),
        in_specs=[vmem] * 2,
        out_specs=(hbm, hbm),
        scratch_shapes=[dma((STORES,)), dma],
        compiler_params=pltpu.CompilerParams(vmem_limit_bytes=4 * 1024 * 1024),
        cost_estimate=pl.CostEstimate(flops=1_000_000_000, bytes_accessed=20_000_000, transcendentals=0),
    )(state, hidden)


def per_device(
    residual_input,
    attention_norm_gain,
    receptance_weight,
    key_weight,
    value_weight,
    decay_weight,
    correction_rate_weight,
    output_gate_weight,
    decay_offset,
    correction_rate_offset,
    self_term_weight,
    head_read_gain,
    previous_state,
    attention_output_weight,
    feedforward_norm_gain,
    routes,
    routing_weight,
    routed_gate_weight,
    routed_up_weight,
    routed_down_weight,
    common_gate_weight,
    common_up_weight,
    common_down_weight,
):
    ep_size = lax.axis_size("ep")
    hidden, state = layer(
        residual_input,
        attention_norm_gain,
        (
            receptance_weight,
            key_weight,
            value_weight,
            decay_weight,
            correction_rate_weight,
            output_gate_weight,
        ),
        routes,
        routing_weight,
        (decay_offset, correction_rate_offset, self_term_weight, head_read_gain),
        previous_state,
        attention_output_weight,
        feedforward_norm_gain,
        (
            common_gate_weight,
            common_up_weight,
            common_down_weight,
            routed_gate_weight[0],
            routed_up_weight[0],
            routed_down_weight[0],
        ),
        ep_size,
    )
    next_state, hidden_out = store(state, hidden)
    return (hidden_out, next_state)


def solution(mesh):
    return jax.shard_map(
        per_device,
        mesh=mesh,
        in_specs=(
            P(("grp", "ep"), None),
            P(),
            P(None, "ep"),
            P(None, "ep"),
            P(None, "ep"),
            P(None, "ep"),
            P(None, "ep"),
            P(None, "ep"),
            P(),
            P(),
            P(),
            P(),
            P(("grp", "ep"), None, None),
            P(),
            P(),
            P("grp", None),
            P("grp", None),
            P("ep", None, None),
            P("ep", None, None),
            P("ep", None, None),
            P(),
            P(),
            P(),
        ),
        out_specs=(P(("grp", "ep"), None), P(("grp", "ep"), None, None)),
        check_vma=False,
    )
```

```python
import functools
import math

import jax
import jax.numpy as jnp
from jax import lax
from jax.experimental import pallas as pl
from jax.experimental.pallas import tpu as pltpu
from jax.sharding import PartitionSpec as P

HEAD_COUNT = 16
HEAD_SIZE = 64
CAP = 4
ROLES = 6
LANES = 128
F32 = jnp.float32
BF16 = jnp.bfloat16


def rms_norm(value_rows, gain):
    scale = lax.rsqrt(jnp.mean(value_rows * value_rows, axis=-1, keepdims=True) + 1e-06)
    return (value_rows * scale * gain.astype(F32)).astype(BF16)


def expert_mlp(rows, gate_w, up_w, down_w):
    gate = jnp.dot(rows, gate_w, preferred_element_type=F32)
    upward = jnp.dot(rows, up_w, preferred_element_type=F32)
    hidden = (jax.nn.silu(gate) * upward).astype(BF16)
    return jnp.dot(hidden, down_w, preferred_element_type=F32).astype(BF16)


def split(value):
    high = value.astype(BF16)
    return high, (value - high.astype(F32)).astype(BF16)


def dot(a, b):
    return jnp.dot(a, b, preferred_element_type=F32)


PLANE = 8
CORES = 2
COLUMNS = PLANE // CORES


def remote(source, target, device, send_sem, recv_sem):
    return pltpu.make_async_remote_copy(
        src_ref=source, dst_ref=target, send_sem=send_sem, recv_sem=recv_sem,
        device_id={"ep": device}, device_id_type=pl.DeviceIdType.MESH,
    )


def route_tables(routes, weights, me, tokens, select_out, coef_out):
    everyone = routes.shape[1]
    slots = select_out.shape[1]
    contract = (((1,), (1,)), ((), ()))
    mine = lax.broadcasted_iota(jnp.int32, (tokens, everyone), 1) - me * tokens
    pick = (mine == lax.broadcasted_iota(jnp.int32, (tokens, everyone), 0)).astype(F32).astype(BF16)

    def own(table):
        return lax.dot_general(pick, table, contract, preferred_element_type=F32)

    named = own(routes.astype(F32).astype(BF16))
    weight_high, weight_low = split(weights)
    own_high, own_low = own(weight_high), own(weight_low)
    lane = lax.broadcasted_iota(jnp.int32, (tokens, slots), 1)
    expert = (lane // CAP).astype(F32)
    hit = jnp.zeros((tokens, slots), F32)
    high, low = hit, hit
    for entry in range(routes.shape[0]):
        match = (named[:, entry : entry + 1] == expert).astype(F32)
        hit = hit + match
        high = high + match * own_high[:, entry : entry + 1]
        low = low + match * own_low[:, entry : entry + 1]
    later = lax.broadcasted_iota(jnp.int32, (tokens, tokens), 0)
    earlier = lax.broadcasted_iota(jnp.int32, (tokens, tokens), 1)
    before = (earlier < later).astype(F32).astype(BF16)
    rank = dot(before, hit.astype(BF16))
    chosen = hit * (rank == (lane % CAP).astype(F32)).astype(F32)
    select_out[...] = chosen
    coef_out[:tokens] = (chosen * high).astype(BF16)
    coef_out[tokens:] = (chosen * low).astype(BF16)


def chosen_tables(routes, me, core, depth, tokens, chosen_ref):
    everyone = routes.shape[1]
    sources = everyone // tokens
    slots, length = chosen_ref.shape[1:]
    iota = lambda shape, axis: lax.broadcasted_iota(jnp.int32, shape, axis)
    flag = lambda value: value.astype(F32)
    hit = jnp.zeros((1, everyone), F32)
    for entry in range(routes.shape[0]):
        hit = hit + flag(routes[entry : entry + 1] == me)
    mine = flag(iota((sources, everyone), 1) // tokens == iota((sources, everyone), 0))
    fold = flag(iota((everyone, tokens), 0) % tokens == iota((everyone, tokens), 1))
    table = dot((mine * hit).astype(BF16), fold.astype(BF16))
    before = flag(iota((tokens, tokens), 0) < iota((tokens, tokens), 1))
    rank = dot(table.astype(BF16), before.astype(BF16))
    unfold = flag(iota((tokens, length), 1) % tokens == iota((tokens, length), 0)).astype(BF16)
    spread_hit = dot(table.astype(BF16), unfold)
    spread_rank = dot(rank.astype(BF16), unfold)
    for group in range(CORES):
        of_core = core if group == 0 else CORES - 1 - core
        block = iota((1, length), 1) // tokens
        source = ((block % depth) * COLUMNS + block // depth) * CORES + of_core
        here = flag(iota((sources, length), 0) == source)
        hits = jnp.sum(here * spread_hit, axis=0, keepdims=True)
        ranks = jnp.sum(here * spread_rank, axis=0, keepdims=True)
        row = iota((slots, length), 0)
        chosen = flag(row // CAP == source) * hits * flag(flag(row % CAP) == ranks)
        chosen_ref[group] = chosen.astype(BF16)


def place_matrix(piece, rows, width):
    lane = lax.broadcasted_iota(jnp.int32, (1, ROLES * LANES), 1)
    inner = lane % HEAD_SIZE - piece * CORES * width
    core = inner // width
    row = (core * ROLES + lane // LANES) * width + inner - core * width
    row = jnp.where((inner >= 0) & (inner < CORES * width), row, -1)
    here = lax.broadcasted_iota(jnp.int32, (rows, ROLES * LANES), 0)
    return (here == row).astype(F32).astype(BF16)


def gather_matrix(first, columns):
    value = first + lax.broadcasted_iota(jnp.int32, (columns, LANES), 0) // HEAD_SIZE
    lane = lax.broadcasted_iota(jnp.int32, (columns, LANES), 1) % HEAD_SIZE
    return (value == lane).astype(F32).astype(BF16)


def spread_matrix(first, columns):
    value = first + lax.broadcasted_iota(jnp.int32, (LANES, columns), 1) // HEAD_SIZE
    row = lax.broadcasted_iota(jnp.int32, (LANES, columns), 0) % HEAD_SIZE
    return (value == row).astype(F32).astype(BF16)


def gain_row(gain):
    rows = gain.astype(F32)
    return jnp.concatenate([rows[i : i + 1] for i in range(rows.shape[0])], axis=1)


PARTS = 4
STORES = 8
UNITS = 2


def layer_kernel(
    depth,
    resid_hbm, gain_hbm, w0, w1, w2, w3, w4, w5, routes_hbm, rweight_hbm,
    const0, const1, const2, const3, state_hbm, out_w_hbm, ffn_gain_hbm, g0, g1, g2, g3, g4, g5,
    hidden_out, state,
    gain, weight, routes, rweight, held, mates, cols, land,
    raw, consts, out_w, ffn_gain, b0, b1, b2, b3, b4, b5,
    place, role_ref, unit_ref, query_ref, mixed_ref, recalled_ref, decay_ref, removal_ref, scaled_ref, select_ref, coef_ref, chosen_ref, base_ref,
    middle_ref, normed_ref, out_rows, served, output, returned,
    load_sem, weight_sem, state_sem, big_sem,
    z_send, z_recv, near_send, near_recv, half_send, half_recv, mate_send, mate_recv, exchange_send, exchange_recv,
    out_send, out_recv, go_send, go_recv, back_send, back_recv,
):
    total = depth * PLANE
    chips = depth * COLUMNS
    tokens, model = resid_hbm.shape
    cut = model // UNITS
    me = lax.axis_index("ep")
    core = lax.rem(me, CORES)
    chip = me // CORES
    column = lax.rem(chip, COLUMNS)
    level = chip // COLUMNS
    x = lax.rem(column, 2)
    y = column // 2
    mate = me + 1 - 2 * core
    column_x = column + 1 - 2 * x
    column_y = column + 2 - 4 * y
    far = COLUMNS - 1 - column
    pieces = land.shape[1]
    rows_all = tokens * HEAD_COUNT

    def device(of_level, of_column):
        return (of_level * COLUMNS + of_column) * CORES + core

    along_x, along_y = device(level, column_x), device(level, column_y)

    barrier = pltpu.get_barrier_semaphore()

    loads = [
        pltpu.make_async_copy(source, target, load_sem.at[i])
        for i, (source, target) in enumerate(
            (
                (resid_hbm.at[:, pl.ds(0, cut)], held.at[column, level, 0]),
                (resid_hbm.at[:, pl.ds(cut, cut)], held.at[column, level, 1]),
                (gain_hbm, gain), (routes_hbm, routes), (rweight_hbm, rweight),
                (const0, raw.at[0]), (const1, raw.at[1]), (const2, raw.at[2]), (const3, raw.at[3]),
                (ffn_gain_hbm, ffn_gain),
            )
        )
    ]
    for load in loads[:2]:
        load.start()

    def greet(number, carry):
        peer = lax.rem(me + number, total)
        pl.semaphore_signal(barrier, inc=1, device_id={"ep": peer}, device_id_type=pl.DeviceIdType.MESH)
        return carry

    lax.fori_loop(1, total, greet, 0)

    for load in loads[2:]:
        load.start()
    weight_loads = [
        pltpu.make_async_copy(source, weight.at[core, i], weight_sem.at[i])
        for i, source in enumerate((w0, w1, w2, w3, w4, w5))
    ]
    for load in weight_loads:
        load.start()
    span = state.shape[2] // PARTS
    state_loads = [
        pltpu.make_async_copy(
            state_hbm.at[:, :, pl.ds(i * span, span)], state.at[:, :, pl.ds(i * span, span)], state_sem.at[i]
        )
        for i in range(PARTS)
    ]
    big_loads = [
        pltpu.make_async_copy(source, target, big_sem.at[i])
        for i, (source, target) in enumerate(
            ((out_w_hbm, out_w), (g0, b0), (g1, b1), (g2, b2), (g3, b3), (g4, b4), (g5, b5))
        )
    ]

    loads[0].wait()
    loads[1].wait()
    pl.semaphore_wait(barrier, total - 1)

    nearer = jnp.minimum(level, depth - 1 - level)

    def nearest(k):
        step = (k + 1) // 2 if k % 2 else -(k // 2)
        beyond = jnp.where(2 * level < depth - 1, k - nearer, nearer - k)
        return level + jnp.where(k <= 2 * nearer, step, beyond)

    order = [level] + [nearest(k) for k in range(1, depth)]

    turns = UNITS // 2

    def along_z(to, slot, half):
        block = held.at[column, slot, half]
        downward = jnp.where(to > level, 0, 1)
        return remote(
            block, block, device(to, column), z_send.at[downward, slot, half], z_recv.at[slot, half]
        )

    def each_way(act):
        for half in range(UNITS):
            for to in (level + 1, level - 1):

                @pl.when((to >= 0) & (to < depth))
                def _():
                    act(along_z(to, level, half))

    def onward(slot, half, act):
        to = jnp.where(slot > level, level - 1, level + 1)

        @pl.when((to >= 0) & (to < depth))
        def _():
            act(along_z(to, slot, half))

    each_way(lambda copy: copy.start())
    sent = []

    def near(axis, of_column, slot, half, target):
        block = held.at[of_column, slot, half]
        return remote(block, block, target, near_send.at[axis, slot, half], near_recv.at[axis, slot, half])

    def forward(slot, half):
        for axis, target in ((0, along_y), (1, along_x)):
            copy = near(axis, column, slot, half if axis == 0 else 1 - half, target)
            copy.start()
            sent.append(copy)

    def relay(slot, turn):
        for axis, (of_column, target) in enumerate(((column_y, along_x), (column_x, along_y))):
            unit = axis * turns + turn
            near(axis, of_column, slot, unit, target).wait_recv()
            block = held.at[of_column, slot, unit]
            copy = remote(block, block, target, half_send.at[slot, unit], half_recv.at[slot, unit])
            copy.start()
            sent.append(copy)

    for half in range(UNITS):
        forward(level, half)
    for load in weight_loads:
        load.wait()
    for load in state_loads + big_loads:
        load.start()
    swap = remote(weight.at[core], weight.at[core], mate, mate_send, mate_recv)
    swap.start()
    for load in loads[2:]:
        load.wait()
    route_tables(routes[...], rweight[...], me, tokens, select_ref, coef_ref)
    chosen_tables(routes[...], me, core, depth, tokens, chosen_ref)
    for number in range(4):
        pair = raw[number]
        turned = pltpu.roll(pair, HEAD_SIZE, 1)
        first = lax.broadcasted_iota(jnp.int32, pair.shape, 1) < HEAD_SIZE
        count = pair.shape[0]
        consts[number, pl.ds(0, count, stride=2), :] = jnp.where(first, pair, turned)
        consts[number, pl.ds(1, count, stride=2), :] = jnp.where(first, turned, pair)
    for piece in range(pieces):
        place[piece] = place_matrix(piece, place.shape[1], weight.shape[2])

    for before, slot in zip(order, order[1:]):
        for half in range(UNITS):
            along_z(level, slot, half).wait_recv()
            onward(slot, half, lambda copy: copy.start())
            if half % 2:
                forward(slot, 0)
                forward(slot, 1)
                relay(before, half // 2)
    swap.wait_recv()

    def compute(of_column, slots):
        sides = [
            jnp.concatenate([held[of_column, slot, half].astype(F32) for slot in slots], axis=0)
            for half in range(UNITS)
        ]
        rows = rms_norm(jnp.concatenate(sides, axis=1), gain_row(gain[...]))
        both = weight[...]
        width = both.shape[2]
        if width % 16:
            both = both.astype(F32)
        both = both.reshape(CORES * ROLES * width, model).astype(BF16)
        result = lax.dot_general(rows, both, (((1,), (1,)), ((), ())), preferred_element_type=F32)
        for i, slot in enumerate(slots):
            cols[of_column, slot] = result[i * tokens : (i + 1) * tokens].astype(BF16)

    def handed(of_level, of_column):
        to_chip = of_level * COLUMNS + of_column
        number = lax.rem(to_chip - chip + chips, chips)
        return remote(
            cols.at[of_column, of_level], land.at[chip // pieces, lax.rem(chip, pieces)], to_chip * CORES + core,
            out_send.at[number], out_recv.at[number],
        )

    def give(of_column, slots):
        for to in slots:
            if of_column is column and to is level:
                land[chip // pieces, lax.rem(chip, pieces)] = cols[column, level]
            else:
                handed(to, of_column).start()

    compute(column, order)
    give(column, order)
    for turn in range(turns):
        relay(order[-1], turn)
    for axis, of_column in ((0, column_y), (1, column_x)):
        for slot in order:
            for turn in range(turns):
                near(axis, of_column, slot, (1 - axis) * turns + turn, along_x).wait_recv()
        compute(of_column, order)
        give(of_column, order)
    exchange = remote(held, mates, mate, exchange_send, exchange_recv)
    for slots in (order[:-1], order[-1:]):
        for slot in slots:
            for unit in range(UNITS):
                block = held.at[far, slot, unit]
                remote(block, block, along_x, half_send.at[slot, unit], half_recv.at[slot, unit]).wait_recv()
        if slots[-1] is order[-1]:
            exchange.start()
        compute(far, slots)
        give(far, slots)

    def finish(number, carry):
        to_chip = lax.rem(chip + number, chips)
        copy = remote(
            cols.at[0, 0], land.at[0, 0], to_chip * CORES + core, out_send.at[number], out_recv.at[number]
        )
        copy.wait_recv()
        copy.wait_send()
        return carry

    lax.fori_loop(1, chips, finish, 0)

    spread_out = jnp.zeros((rows_all, ROLES * LANES), F32)
    for piece in range(pieces):
        rows = land[:, piece].astype(F32).reshape(rows_all, land.shape[3]).astype(BF16)
        spread_out = spread_out + dot(rows, place[piece])
    for head in range(HEAD_COUNT):
        for number in range(ROLES):
            part = spread_out[head * tokens : (head + 1) * tokens, number * LANES : (number + 1) * LANES]
            role_ref[number, pl.ds(head, tokens, stride=HEAD_COUNT), :] = part

    def const(number):
        one = consts[number]
        return jnp.concatenate([one] * tokens, axis=0)

    half_lanes = HEAD_SIZE / LANES

    def head_sum(value):
        return jnp.sum(value, axis=-1, keepdims=True) * half_lanes

    receptance, keys, values = role_ref[0], role_ref[1], role_ref[2]
    decay = jnp.exp(-math.exp(-0.5) * jax.nn.sigmoid(const(0) + role_ref[3]))
    rate = jax.nn.sigmoid(const(1) + role_ref[4])
    unit_key = keys * lax.rsqrt(1.0 + head_sum(keys * keys))
    scaled_key = keys * rate
    removal = unit_key * rate
    self_sum = head_sum(receptance * scaled_key * const(2))
    removed = head_sum(removal * receptance)
    added = head_sum(scaled_key * receptance)
    unit_ref[...] = unit_key
    query_ref[...] = decay * receptance
    decay_ref[...] = decay
    removal_ref[...] = removal
    scaled_ref[...] = scaled_key

    recalled = jnp.zeros((rows_all, LANES), F32)
    kept = jnp.zeros((rows_all, LANES), F32)
    for part in range(PARTS):
        state_loads[part].wait()
        pick = gather_matrix(part * span // HEAD_SIZE, span)
        block = state[:, :, part * span : (part + 1) * span].reshape(rows_all, span)
        wide_key = jnp.concatenate([unit_ref[...]] * (span // LANES), axis=1)
        recalled = recalled + dot((block * wide_key).astype(BF16), pick)
        wide_query = jnp.concatenate([query_ref[...]] * (span // LANES), axis=1)
        kept = kept + dot((block * wide_query).astype(BF16), pick)
    recalled_ref[...] = recalled
    values = role_ref[2]
    read = kept - recalled * removed + values * added
    centered = read - head_sum(read) * (1.0 / HEAD_SIZE)
    variance = head_sum(centered * centered) * (1.0 / HEAD_SIZE)
    normal = centered * lax.rsqrt(variance + 0.00064) * const(3)
    mixed_ref[...] = (normal + self_sum * values) * jax.nn.sigmoid(role_ref[5])

    lane = lax.broadcasted_iota(jnp.int32, (tokens, LANES), 1)
    per = LANES // HEAD_SIZE
    parts = []
    for first in range(0, HEAD_COUNT, per):
        part = mixed_ref[pl.ds(first, tokens, stride=HEAD_COUNT), :]
        for other in range(1, per):
            rest = mixed_ref[pl.ds(first + other, tokens, stride=HEAD_COUNT), :]
            part = jnp.where(lane < other * HEAD_SIZE, part, rest)
        parts.append(part.astype(BF16))
    mixed = jnp.concatenate(parts, axis=1)
    picked = lax.dot_general(
        select_ref[...].astype(BF16), mixed, (((0,), (0,)), ((), ())), preferred_element_type=F32
    )
    out_rows[...] = picked.reshape(out_rows.shape).astype(BF16)

    def go(number):
        to = lax.rem(me + number, total)
        return remote(out_rows.at[to], served.at[me], to, go_send.at[number], go_recv.at[number])

    def back(to):
        number = lax.rem(to - me + total, total)
        return remote(output.at[to], returned.at[me], to, back_send.at[number], back_recv.at[number])

    place_in_plane = lax.rem(me, PLANE)

    def launch(of_level):
        def one(i, carry):
            to = of_level * PLANE + lax.rem(place_in_plane + i, PLANE)

            @pl.when(to != me)
            def _():
                go(lax.rem(to - me + total, total)).start()

            return carry

        lax.fori_loop(0, PLANE, one, 0)

    for of_level in order[::-1]:
        launch(of_level)
    served[me] = out_rows[me]
    big_loads[0].wait()
    attended = dot(mixed, out_w[...]).astype(BF16).astype(F32)
    own_rows = jnp.concatenate([held[column, level, half] for half in range(UNITS)], axis=1)
    middle = own_rows.astype(F32) + attended
    middle_ref[...] = middle
    normed_ref[...] = rms_norm(middle, gain_row(ffn_gain[...]))
    exchange.wait_recv()
    for half in range(UNITS):
        base = jnp.zeros((total * CAP, cut), F32)
        for group, source in ((0, held), (1, mates)):
            rows = source[:, :, half].astype(F32).reshape(chips * tokens, cut).astype(BF16)
            base = base + dot(chosen_ref[group], rows)
        base_ref[:, half * cut : (half + 1) * cut] = base.astype(BF16)
    for load in big_loads[1:4]:
        load.wait()
    shared = expert_mlp(normed_ref[...], b0[...], b1[...], b2[...])
    middle_ref[...] = middle_ref[...] + shared.astype(F32)
    for load in big_loads[4:]:
        load.wait()

    for of_level in order[::-1]:
        first = of_level * PLANE

        def arrive(i, carry):
            source = first + i

            @pl.when(source != me)
            def _():
                go(lax.rem(me - source + total, total)).wait_recv()

            return carry

        lax.fori_loop(0, PLANE, arrive, 0)
        rows = served[pl.ds(first, PLANE)].reshape(PLANE * CAP, served.shape[2])
        projected = dot(rows, out_w[...]).astype(BF16).astype(F32)
        below = base_ref[pl.ds(pl.multiple_of(first * CAP, PLANE * CAP), PLANE * CAP), :]
        rows = rms_norm(below.astype(F32) + projected, gain_row(ffn_gain[...]))
        result = expert_mlp(rows, b3[...], b4[...], b5[...])
        output[pl.ds(first, PLANE)] = result.reshape(PLANE, CAP, model)

        def give_back(i, carry):
            source = first + i

            @pl.when(source != me)
            def _():
                back(source).start()

            return carry

        lax.fori_loop(0, PLANE, give_back, 0)
    own_lane = lax.broadcasted_iota(jnp.int32, (rows_all, LANES), 1) < HEAD_SIZE
    high, low = split(recalled_ref[...])
    both = jnp.where(own_lane, high.astype(F32), low.astype(F32)).astype(BF16)
    alone = jnp.where(own_lane, role_ref[2], 0.0).astype(BF16)
    stacked = jnp.concatenate([both, alone], axis=0)
    step = 4 * HEAD_SIZE

    def twice(ref):
        return jnp.concatenate([ref[...]] * (step // LANES), axis=1)

    for first in range(0, state.shape[2], step):
        spread = dot(stacked, spread_matrix(first // HEAD_SIZE, step))
        block = state[:, :, first : first + step].reshape(rows_all, step)
        new = block * twice(decay_ref) - spread[:rows_all] * twice(removal_ref)
        new = new + spread[rows_all:] * twice(scaled_ref)
        state[:, :, first : first + step] = new.reshape(tokens, HEAD_COUNT, step)

    returned[me] = output[me]

    def ended(number, carry):
        go(number).wait_send()
        copy = back(lax.rem(me + number, total))
        copy.wait_recv()
        copy.wait_send()
        return carry

    lax.fori_loop(1, total, ended, 0)
    routed = dot(coef_ref[...], returned[...].reshape(total * CAP, model))
    hidden_out[...] = (middle_ref[...] + (routed[:tokens] + routed[tokens:])).astype(BF16)

    each_way(lambda copy: copy.wait_send())
    for slot in order[1:]:
        for half in range(UNITS):
            onward(slot, half, lambda copy: copy.wait_send())
    for copy in sent:
        copy.wait_send()
    swap.wait_send()
    exchange.wait_send()


def layer(resid, gain, weights, routes, routing_weight, consts, state, out_w, ffn_gain, experts, ep_size):
    depth = ep_size // PLANE
    chips = ep_size // CORES
    pieces = chips // HEAD_COUNT
    tokens, model = resid.shape
    weights = [w.T for w in weights]
    width = weights[0].shape[0]
    wide = CORES * ROLES * width
    rows_all = tokens * HEAD_COUNT
    routes, routing_weight = routes.T, routing_weight.T
    gain = gain.reshape(model // LANES, LANES)
    ffn_gain = ffn_gain.reshape(model // LANES, LANES)
    consts = [c.reshape(-1, LANES) for c in consts]
    slots = ep_size * CAP
    dma = pltpu.SemaphoreType.DMA
    hbm = pl.BlockSpec(memory_space=pltpu.HBM)
    vmem = pl.BlockSpec(memory_space=pltpu.VMEM)
    operands = (resid, gain, *weights, routes, routing_weight, *consts, state, out_w, ffn_gain, *experts)
    operands = [pltpu.with_memory_space_constraint(a, pltpu.HBM) for a in operands]
    return pl.pallas_call(
        functools.partial(layer_kernel, depth),
        out_shape=(jax.ShapeDtypeStruct((tokens, model), BF16), jax.ShapeDtypeStruct(state.shape, F32)),
        in_specs=[hbm] * len(operands),
        out_specs=(vmem,) * 2,
        scratch_shapes=[
            pltpu.VMEM(gain.shape, BF16),
            pltpu.VMEM((CORES, ROLES, width, model), BF16),
            pltpu.VMEM(routes.shape, jnp.int32),
            pltpu.VMEM(routes.shape, F32),
            pltpu.VMEM((COLUMNS, depth, UNITS, tokens, model // UNITS), BF16),
            pltpu.VMEM((COLUMNS, depth, UNITS, tokens, model // UNITS), BF16),
            pltpu.VMEM((COLUMNS, depth, tokens, wide), BF16),
            pltpu.VMEM((HEAD_COUNT, pieces, tokens, wide), BF16),
            pltpu.VMEM((4,) + consts[0].shape, F32),
            pltpu.VMEM((4, HEAD_COUNT, LANES), F32),
            pltpu.VMEM(out_w.shape, BF16),
            pltpu.VMEM(gain.shape, BF16),
        ]
        + [pltpu.VMEM(w.shape, BF16) for w in experts]
        + [
            pltpu.VMEM((pieces, wide, ROLES * LANES), BF16),
            pltpu.VMEM((ROLES, rows_all, LANES), F32),
        ]
        + [pltpu.VMEM((rows_all, LANES), F32)] * 7
        + [
            pltpu.VMEM((tokens, slots), F32),
            pltpu.VMEM((2 * tokens, slots), BF16),
            pltpu.VMEM((CORES, slots, chips * tokens), BF16),
            pltpu.VMEM((slots, model), BF16),
            pltpu.VMEM((tokens, model), F32),
            pltpu.VMEM((tokens, model), BF16),
        ]
        + [pltpu.VMEM((ep_size, CAP, out_w.shape[0]), BF16)] * 2
        + [pltpu.VMEM((ep_size, CAP, model), BF16)] * 2
        + [
            dma((10,)), dma((ROLES,)), dma((PARTS,)), dma((7,)),
            dma((2, depth, UNITS)), dma((depth, UNITS)),
            dma((2, depth, UNITS)), dma((2, depth, UNITS)),
            dma((depth, UNITS)), dma((depth, UNITS)),
            dma, dma, dma, dma,
            dma((chips,)), dma((chips,)),
        ]
        + [dma((ep_size,))] * 4,
        compiler_params=pltpu.CompilerParams(
            has_side_effects=True, collective_id=0, vmem_limit_bytes=46 * 1024 * 1024
        ),
        cost_estimate=pl.CostEstimate(flops=30_000_000_000, bytes_accessed=100_000_000, transcendentals=0),
    )(*operands)


def store_kernel(state, hidden, next_hbm, hidden_hbm, next_sem, hidden_sem):
    parts = next_sem.shape[0]
    group = state.shape[0] // parts
    copies = [pltpu.make_async_copy(hidden, hidden_hbm, hidden_sem)]
    for part in range(parts):
        here = pl.ds(part * group, group)
        copies.append(pltpu.make_async_copy(state.at[here], next_hbm.at[here], next_sem.at[part]))
    for copy in copies:
        copy.start()
    for copy in copies:
        copy.wait()


def store(state, hidden):
    vmem = pl.BlockSpec(memory_space=pltpu.VMEM)
    hbm = pl.BlockSpec(memory_space=pltpu.HBM)
    dma = pltpu.SemaphoreType.DMA
    return pl.pallas_call(
        store_kernel,
        out_shape=(jax.ShapeDtypeStruct(state.shape, F32), jax.ShapeDtypeStruct(hidden.shape, BF16)),
        in_specs=[vmem] * 2,
        out_specs=(hbm, hbm),
        scratch_shapes=[dma((STORES,)), dma],
        compiler_params=pltpu.CompilerParams(vmem_limit_bytes=4 * 1024 * 1024),
        cost_estimate=pl.CostEstimate(flops=1_000_000_000, bytes_accessed=20_000_000, transcendentals=0),
    )(state, hidden)


def per_device(
    residual_input,
    attention_norm_gain,
    receptance_weight,
    key_weight,
    value_weight,
    decay_weight,
    correction_rate_weight,
    output_gate_weight,
    decay_offset,
    correction_rate_offset,
    self_term_weight,
    head_read_gain,
    previous_state,
    attention_output_weight,
    feedforward_norm_gain,
    routes,
    routing_weight,
    routed_gate_weight,
    routed_up_weight,
    routed_down_weight,
    common_gate_weight,
    common_up_weight,
    common_down_weight,
):
    ep_size = lax.axis_size("ep")
    hidden, state = layer(
        residual_input,
        attention_norm_gain,
        (
            receptance_weight,
            key_weight,
            value_weight,
            decay_weight,
            correction_rate_weight,
            output_gate_weight,
        ),
        routes,
        routing_weight,
        (decay_offset, correction_rate_offset, self_term_weight, head_read_gain),
        previous_state,
        attention_output_weight,
        feedforward_norm_gain,
        (
            common_gate_weight,
            common_up_weight,
            common_down_weight,
            routed_gate_weight[0],
            routed_up_weight[0],
            routed_down_weight[0],
        ),
        ep_size,
    )
    next_state, hidden_out = store(state, hidden)
    return (hidden_out, next_state)


def solution(mesh):
    return jax.shard_map(
        per_device,
        mesh=mesh,
        in_specs=(
            P(("grp", "ep"), None),
            P(),
            P(None, "ep"),
            P(None, "ep"),
            P(None, "ep"),
            P(None, "ep"),
            P(None, "ep"),
            P(None, "ep"),
            P(),
            P(),
            P(),
            P(),
            P(("grp", "ep"), None, None),
            P(),
            P(),
            P("grp", None),
            P("grp", None),
            P("ep", None, None),
            P("ep", None, None),
            P("ep", None, None),
            P(),
            P(),
            P(),
        ),
        out_specs=(P(("grp", "ep"), None), P(("grp", "ep"), None, None)),
        check_vma=False,
    )
```

```python
import functools
import math

import jax
import jax.numpy as jnp
from jax import lax
from jax.experimental import pallas as pl
from jax.experimental.pallas import tpu as pltpu
from jax.sharding import PartitionSpec as P

HEAD_COUNT = 16
HEAD_SIZE = 64
CAP = 4
ROLES = 6
LANES = 128
F32 = jnp.float32
BF16 = jnp.bfloat16


def rms_norm(value_rows, gain):
    scale = lax.rsqrt(jnp.mean(value_rows * value_rows, axis=-1, keepdims=True) + 1e-06)
    return (value_rows * scale * gain.astype(F32)).astype(BF16)


def expert_mlp(rows, gate_w, up_w, down_w):
    gate = jnp.dot(rows, gate_w, preferred_element_type=F32)
    upward = jnp.dot(rows, up_w, preferred_element_type=F32)
    hidden = (jax.nn.silu(gate) * upward).astype(BF16)
    return jnp.dot(hidden, down_w, preferred_element_type=F32).astype(BF16)


def split(value):
    high = value.astype(BF16)
    return high, (value - high.astype(F32)).astype(BF16)


def dot(a, b):
    return jnp.dot(a, b, preferred_element_type=F32)


PLANE = 8
CORES = 2
COLUMNS = PLANE // CORES


def remote(source, target, device, send_sem, recv_sem):
    return pltpu.make_async_remote_copy(
        src_ref=source, dst_ref=target, send_sem=send_sem, recv_sem=recv_sem,
        device_id={"ep": device}, device_id_type=pl.DeviceIdType.MESH,
    )


def route_tables(routes, weights, me, tokens, select_out, coef_out):
    everyone = routes.shape[1]
    slots = select_out.shape[1]
    contract = (((1,), (1,)), ((), ()))
    mine = lax.broadcasted_iota(jnp.int32, (tokens, everyone), 1) - me * tokens
    pick = (mine == lax.broadcasted_iota(jnp.int32, (tokens, everyone), 0)).astype(F32).astype(BF16)

    def own(table):
        return lax.dot_general(pick, table, contract, preferred_element_type=F32)

    named = own(routes.astype(F32).astype(BF16))
    weight_high, weight_low = split(weights)
    own_high, own_low = own(weight_high), own(weight_low)
    lane = lax.broadcasted_iota(jnp.int32, (tokens, slots), 1)
    expert = (lane // CAP).astype(F32)
    hit = jnp.zeros((tokens, slots), F32)
    high, low = hit, hit
    for entry in range(routes.shape[0]):
        match = (named[:, entry : entry + 1] == expert).astype(F32)
        hit = hit + match
        high = high + match * own_high[:, entry : entry + 1]
        low = low + match * own_low[:, entry : entry + 1]
    later = lax.broadcasted_iota(jnp.int32, (tokens, tokens), 0)
    earlier = lax.broadcasted_iota(jnp.int32, (tokens, tokens), 1)
    before = (earlier < later).astype(F32).astype(BF16)
    rank = dot(before, hit.astype(BF16))
    chosen = hit * (rank == (lane % CAP).astype(F32)).astype(F32)
    select_out[...] = chosen
    coef_out[:tokens] = (chosen * high).astype(BF16)
    coef_out[tokens:] = (chosen * low).astype(BF16)


def chosen_tables(routes, me, core, depth, tokens, chosen_ref):
    everyone = routes.shape[1]
    sources = everyone // tokens
    slots, length = chosen_ref.shape[1:]
    iota = lambda shape, axis: lax.broadcasted_iota(jnp.int32, shape, axis)
    flag = lambda value: value.astype(F32)
    hit = jnp.zeros((1, everyone), F32)
    for entry in range(routes.shape[0]):
        hit = hit + flag(routes[entry : entry + 1] == me)
    mine = flag(iota((sources, everyone), 1) // tokens == iota((sources, everyone), 0))
    fold = flag(iota((everyone, tokens), 0) % tokens == iota((everyone, tokens), 1))
    table = dot((mine * hit).astype(BF16), fold.astype(BF16))
    before = flag(iota((tokens, tokens), 0) < iota((tokens, tokens), 1))
    rank = dot(table.astype(BF16), before.astype(BF16))
    unfold = flag(iota((tokens, length), 1) % tokens == iota((tokens, length), 0)).astype(BF16)
    spread_hit = dot(table.astype(BF16), unfold)
    spread_rank = dot(rank.astype(BF16), unfold)
    for group in range(CORES):
        of_core = core if group == 0 else CORES - 1 - core
        block = iota((1, length), 1) // tokens
        source = ((block % depth) * COLUMNS + block // depth) * CORES + of_core
        here = flag(iota((sources, length), 0) == source)
        hits = jnp.sum(here * spread_hit, axis=0, keepdims=True)
        ranks = jnp.sum(here * spread_rank, axis=0, keepdims=True)
        row = iota((slots, length), 0)
        chosen = flag(row // CAP == source) * hits * flag(flag(row % CAP) == ranks)
        chosen_ref[group] = chosen.astype(BF16)


def place_matrix(piece, rows, width):
    lane = lax.broadcasted_iota(jnp.int32, (1, ROLES * LANES), 1)
    inner = lane % HEAD_SIZE - piece * CORES * width
    core = inner // width
    row = (core * ROLES + lane // LANES) * width + inner - core * width
    row = jnp.where((inner >= 0) & (inner < CORES * width), row, -1)
    here = lax.broadcasted_iota(jnp.int32, (rows, ROLES * LANES), 0)
    return (here == row).astype(F32).astype(BF16)


def gather_matrix(first, columns):
    value = first + lax.broadcasted_iota(jnp.int32, (columns, LANES), 0) // HEAD_SIZE
    lane = lax.broadcasted_iota(jnp.int32, (columns, LANES), 1) % HEAD_SIZE
    return (value == lane).astype(F32).astype(BF16)


def spread_matrix(first, columns):
    value = first + lax.broadcasted_iota(jnp.int32, (LANES, columns), 1) // HEAD_SIZE
    row = lax.broadcasted_iota(jnp.int32, (LANES, columns), 0) % HEAD_SIZE
    return (value == row).astype(F32).astype(BF16)


def gain_row(gain):
    rows = gain.astype(F32)
    return jnp.concatenate([rows[i : i + 1] for i in range(rows.shape[0])], axis=1)


PARTS = 4
STORES = 8
UNITS = 2


def layer_kernel(
    depth,
    resid_hbm, gain_hbm, w0, w1, w2, w3, w4, w5, routes_hbm, rweight_hbm,
    const0, const1, const2, const3, state_hbm, out_w_hbm, ffn_gain_hbm, g0, g1, g2, g3, g4, g5,
    hidden_out, state,
    gain, weight, routes, rweight, held, mates, cols, land,
    raw, consts, out_w, ffn_gain, b0, b1, b2, b3, b4, b5,
    place, role_ref, unit_ref, query_ref, mixed_ref, recalled_ref, decay_ref, removal_ref, scaled_ref, select_ref, coef_ref, chosen_ref, base_ref,
    middle_ref, normed_ref, out_rows, served, output, returned,
    load_sem, weight_sem, state_sem, big_sem,
    z_send, z_recv, near_send, near_recv, half_send, half_recv, mate_send, mate_recv, exchange_send, exchange_recv,
    out_send, out_recv, go_send, go_recv, back_send, back_recv,
):
    total = depth * PLANE
    chips = depth * COLUMNS
    tokens, model = resid_hbm.shape
    cut = model // UNITS
    me = lax.axis_index("ep")
    core = lax.rem(me, CORES)
    chip = me // CORES
    column = lax.rem(chip, COLUMNS)
    level = chip // COLUMNS
    x = lax.rem(column, 2)
    y = column // 2
    mate = me + 1 - 2 * core
    column_x = column + 1 - 2 * x
    column_y = column + 2 - 4 * y
    far = COLUMNS - 1 - column
    pieces = land.shape[1]
    rows_all = tokens * HEAD_COUNT

    def device(of_level, of_column):
        return (of_level * COLUMNS + of_column) * CORES + core

    along_x, along_y = device(level, column_x), device(level, column_y)

    barrier = pltpu.get_barrier_semaphore()

    loads = [
        pltpu.make_async_copy(source, target, load_sem.at[i])
        for i, (source, target) in enumerate(
            (
                (resid_hbm.at[:, pl.ds(0, cut)], held.at[column, level, 0]),
                (resid_hbm.at[:, pl.ds(cut, cut)], held.at[column, level, 1]),
                (gain_hbm, gain), (routes_hbm, routes), (rweight_hbm, rweight),
                (const0, raw.at[0]), (const1, raw.at[1]), (const2, raw.at[2]), (const3, raw.at[3]),
                (ffn_gain_hbm, ffn_gain),
            )
        )
    ]
    for load in loads[:2]:
        load.start()

    def greet(number, carry):
        peer = lax.rem(me + number, total)
        pl.semaphore_signal(barrier, inc=1, device_id={"ep": peer}, device_id_type=pl.DeviceIdType.MESH)
        return carry

    lax.fori_loop(1, total, greet, 0)

    for load in loads[2:]:
        load.start()
    weight_loads = [
        pltpu.make_async_copy(source, weight.at[core, i], weight_sem.at[i])
        for i, source in enumerate((w0, w1, w2, w3, w4, w5))
    ]
    for load in weight_loads:
        load.start()
    span = state.shape[2] // PARTS
    state_loads = [
        pltpu.make_async_copy(
            state_hbm.at[:, :, pl.ds(i * span, span)], state.at[:, :, pl.ds(i * span, span)], state_sem.at[i]
        )
        for i in range(PARTS)
    ]
    big_loads = [
        pltpu.make_async_copy(source, target, big_sem.at[i])
        for i, (source, target) in enumerate(
            ((out_w_hbm, out_w), (g0, b0), (g1, b1), (g2, b2), (g3, b3), (g4, b4), (g5, b5))
        )
    ]

    loads[0].wait()
    loads[1].wait()
    pl.semaphore_wait(barrier, total - 1)

    nearer = jnp.minimum(level, depth - 1 - level)

    def nearest(k):
        step = (k + 1) // 2 if k % 2 else -(k // 2)
        beyond = jnp.where(2 * level < depth - 1, k - nearer, nearer - k)
        return level + jnp.where(k <= 2 * nearer, step, beyond)

    order = [level] + [nearest(k) for k in range(1, depth)]

    turns = UNITS // 2

    def along_z(to, slot, half):
        block = held.at[column, slot, half]
        downward = jnp.where(to > level, 0, 1)
        return remote(
            block, block, device(to, column), z_send.at[downward, slot, half], z_recv.at[slot, half]
        )

    def each_way(act):
        for half in range(UNITS):
            for to in (level + 1, level - 1):

                @pl.when((to >= 0) & (to < depth))
                def _():
                    act(along_z(to, level, half))

    def onward(slot, half, act):
        to = jnp.where(slot > level, level - 1, level + 1)

        @pl.when((to >= 0) & (to < depth))
        def _():
            act(along_z(to, slot, half))

    each_way(lambda copy: copy.start())
    sent = []

    def near(axis, of_column, slot, half, target):
        block = held.at[of_column, slot, half]
        return remote(block, block, target, near_send.at[axis, slot, half], near_recv.at[axis, slot, half])

    def forward(slot, half):
        for axis, target in ((0, along_y), (1, along_x)):
            copy = near(axis, column, slot, half if axis == 0 else 1 - half, target)
            copy.start()
            sent.append(copy)

    def relay(slot, turn):
        for axis, (of_column, target) in enumerate(((column_y, along_x), (column_x, along_y))):
            unit = axis * turns + turn
            near(axis, of_column, slot, unit, target).wait_recv()
            block = held.at[of_column, slot, unit]
            copy = remote(block, block, target, half_send.at[slot, unit], half_recv.at[slot, unit])
            copy.start()
            sent.append(copy)

    for half in range(UNITS):
        forward(level, half)
    for load in weight_loads:
        load.wait()
    for load in state_loads + big_loads:
        load.start()
    swap = remote(weight.at[core], weight.at[core], mate, mate_send, mate_recv)
    swap.start()
    for load in loads[2:]:
        load.wait()
    route_tables(routes[...], rweight[...], me, tokens, select_ref, coef_ref)
    chosen_tables(routes[...], me, core, depth, tokens, chosen_ref)
    for number in range(4):
        pair = raw[number]
        turned = pltpu.roll(pair, HEAD_SIZE, 1)
        first = lax.broadcasted_iota(jnp.int32, pair.shape, 1) < HEAD_SIZE
        count = pair.shape[0]
        consts[number, pl.ds(0, count, stride=2), :] = jnp.where(first, pair, turned)
        consts[number, pl.ds(1, count, stride=2), :] = jnp.where(first, turned, pair)
    for piece in range(pieces):
        place[piece] = place_matrix(piece, place.shape[1], weight.shape[2])

    for before, slot in zip(order, order[1:]):
        for half in range(UNITS):
            along_z(level, slot, half).wait_recv()
            onward(slot, half, lambda copy: copy.start())
            if half % 2:
                forward(slot, 0)
                forward(slot, 1)
                relay(before, half // 2)
    swap.wait_recv()

    def compute(of_column, slots):
        sides = [
            jnp.concatenate([held[of_column, slot, half].astype(F32) for slot in slots], axis=0)
            for half in range(UNITS)
        ]
        rows = rms_norm(jnp.concatenate(sides, axis=1), gain_row(gain[...]))
        both = weight[...]
        width = both.shape[2]
        if width % 16:
            both = both.astype(F32)
        both = both.reshape(CORES * ROLES * width, model).astype(BF16)
        result = lax.dot_general(rows, both, (((1,), (1,)), ((), ())), preferred_element_type=F32)
        for i, slot in enumerate(slots):
            cols[of_column, slot] = result[i * tokens : (i + 1) * tokens].astype(BF16)

    def handed(of_level, of_column):
        to_chip = of_level * COLUMNS + of_column
        number = lax.rem(to_chip - chip + chips, chips)
        return remote(
            cols.at[of_column, of_level], land.at[chip // pieces, lax.rem(chip, pieces)], to_chip * CORES + core,
            out_send.at[number], out_recv.at[number],
        )

    def give(of_column, slots):
        for to in slots:
            if of_column is column and to is level:
                land[chip // pieces, lax.rem(chip, pieces)] = cols[column, level]
            else:
                handed(to, of_column).start()

    compute(column, order)
    give(column, order)
    for turn in range(turns):
        relay(order[-1], turn)
    for axis, of_column in ((0, column_y), (1, column_x)):
        for slot in order:
            for turn in range(turns):
                near(axis, of_column, slot, (1 - axis) * turns + turn, along_x).wait_recv()
        compute(of_column, order)
        give(of_column, order)
    exchange = remote(held, mates, mate, exchange_send, exchange_recv)
    for slots in (order[:-1], order[-1:]):
        for slot in slots:
            for unit in range(UNITS):
                block = held.at[far, slot, unit]
                remote(block, block, along_x, half_send.at[slot, unit], half_recv.at[slot, unit]).wait_recv()
        compute(far, slots)
        give(far, slots)

    def finish(number, carry):
        to_chip = lax.rem(chip + number, chips)
        copy = remote(
            cols.at[0, 0], land.at[0, 0], to_chip * CORES + core, out_send.at[number], out_recv.at[number]
        )
        copy.wait_recv()
        copy.wait_send()
        return carry

    lax.fori_loop(1, chips, finish, 0)
    exchange.start()

    spread_out = jnp.zeros((rows_all, ROLES * LANES), F32)
    for piece in range(pieces):
        rows = land[:, piece].astype(F32).reshape(rows_all, land.shape[3]).astype(BF16)
        spread_out = spread_out + dot(rows, place[piece])
    for head in range(HEAD_COUNT):
        for number in range(ROLES):
            part = spread_out[head * tokens : (head + 1) * tokens, number * LANES : (number + 1) * LANES]
            role_ref[number, pl.ds(head, tokens, stride=HEAD_COUNT), :] = part

    def const(number):
        one = consts[number]
        return jnp.concatenate([one] * tokens, axis=0)

    half_lanes = HEAD_SIZE / LANES

    def head_sum(value):
        return jnp.sum(value, axis=-1, keepdims=True) * half_lanes

    receptance, keys, values = role_ref[0], role_ref[1], role_ref[2]
    decay = jnp.exp(-math.exp(-0.5) * jax.nn.sigmoid(const(0) + role_ref[3]))
    rate = jax.nn.sigmoid(const(1) + role_ref[4])
    unit_key = keys * lax.rsqrt(1.0 + head_sum(keys * keys))
    scaled_key = keys * rate
    removal = unit_key * rate
    self_sum = head_sum(receptance * scaled_key * const(2))
    removed = head_sum(removal * receptance)
    added = head_sum(scaled_key * receptance)
    unit_ref[...] = unit_key
    query_ref[...] = decay * receptance
    decay_ref[...] = decay
    removal_ref[...] = removal
    scaled_ref[...] = scaled_key

    recalled = jnp.zeros((rows_all, LANES), F32)
    kept = jnp.zeros((rows_all, LANES), F32)
    for part in range(PARTS):
        state_loads[part].wait()
        pick = gather_matrix(part * span // HEAD_SIZE, span)
        block = state[:, :, part * span : (part + 1) * span].reshape(rows_all, span)
        wide_key = jnp.concatenate([unit_ref[...]] * (span // LANES), axis=1)
        recalled = recalled + dot((block * wide_key).astype(BF16), pick)
        wide_query = jnp.concatenate([query_ref[...]] * (span // LANES), axis=1)
        kept = kept + dot((block * wide_query).astype(BF16), pick)
    recalled_ref[...] = recalled
    values = role_ref[2]
    read = kept - recalled * removed + values * added
    centered = read - head_sum(read) * (1.0 / HEAD_SIZE)
    variance = head_sum(centered * centered) * (1.0 / HEAD_SIZE)
    normal = centered * lax.rsqrt(variance + 0.00064) * const(3)
    mixed_ref[...] = (normal + self_sum * values) * jax.nn.sigmoid(role_ref[5])

    lane = lax.broadcasted_iota(jnp.int32, (tokens, LANES), 1)
    per = LANES // HEAD_SIZE
    parts = []
    for first in range(0, HEAD_COUNT, per):
        part = mixed_ref[pl.ds(first, tokens, stride=HEAD_COUNT), :]
        for other in range(1, per):
            rest = mixed_ref[pl.ds(first + other, tokens, stride=HEAD_COUNT), :]
            part = jnp.where(lane < other * HEAD_SIZE, part, rest)
        parts.append(part.astype(BF16))
    mixed = jnp.concatenate(parts, axis=1)
    picked = lax.dot_general(
        select_ref[...].astype(BF16), mixed, (((0,), (0,)), ((), ())), preferred_element_type=F32
    )
    out_rows[...] = picked.reshape(out_rows.shape).astype(BF16)

    def go(number):
        to = lax.rem(me + number, total)
        return remote(out_rows.at[to], served.at[me], to, go_send.at[number], go_recv.at[number])

    def back(to):
        number = lax.rem(to - me + total, total)
        return remote(output.at[to], returned.at[me], to, back_send.at[number], back_recv.at[number])

    place_in_plane = lax.rem(me, PLANE)

    def launch(of_level):
        def one(i, carry):
            to = of_level * PLANE + lax.rem(place_in_plane + i, PLANE)

            @pl.when(to != me)
            def _():
                go(lax.rem(to - me + total, total)).start()

            return carry

        lax.fori_loop(0, PLANE, one, 0)

    for of_level in order[::-1]:
        launch(of_level)
    served[me] = out_rows[me]
    big_loads[0].wait()
    attended = dot(mixed, out_w[...]).astype(BF16).astype(F32)
    own_rows = jnp.concatenate([held[column, level, half] for half in range(UNITS)], axis=1)
    middle = own_rows.astype(F32) + attended
    middle_ref[...] = middle
    normed_ref[...] = rms_norm(middle, gain_row(ffn_gain[...]))
    exchange.wait_recv()
    for half in range(UNITS):
        base = jnp.zeros((total * CAP, cut), F32)
        for group, source in ((0, held), (1, mates)):
            rows = source[:, :, half].astype(F32).reshape(chips * tokens, cut).astype(BF16)
            base = base + dot(chosen_ref[group], rows)
        base_ref[:, half * cut : (half + 1) * cut] = base.astype(BF16)
    for load in big_loads[1:4]:
        load.wait()
    shared = expert_mlp(normed_ref[...], b0[...], b1[...], b2[...])
    middle_ref[...] = middle_ref[...] + shared.astype(F32)
    for load in big_loads[4:]:
        load.wait()

    for of_level in order[::-1]:
        first = of_level * PLANE

        def arrive(i, carry):
            source = first + i

            @pl.when(source != me)
            def _():
                go(lax.rem(me - source + total, total)).wait_recv()

            return carry

        lax.fori_loop(0, PLANE, arrive, 0)
        rows = served[pl.ds(first, PLANE)].reshape(PLANE * CAP, served.shape[2])
        projected = dot(rows, out_w[...]).astype(BF16).astype(F32)
        below = base_ref[pl.ds(pl.multiple_of(first * CAP, PLANE * CAP), PLANE * CAP), :]
        rows = rms_norm(below.astype(F32) + projected, gain_row(ffn_gain[...]))
        result = expert_mlp(rows, b3[...], b4[...], b5[...])
        output[pl.ds(first, PLANE)] = result.reshape(PLANE, CAP, model)

        def give_back(i, carry):
            source = first + i

            @pl.when(source != me)
            def _():
                back(source).start()

            return carry

        lax.fori_loop(0, PLANE, give_back, 0)
    own_lane = lax.broadcasted_iota(jnp.int32, (rows_all, LANES), 1) < HEAD_SIZE
    high, low = split(recalled_ref[...])
    both = jnp.where(own_lane, high.astype(F32), low.astype(F32)).astype(BF16)
    alone = jnp.where(own_lane, role_ref[2], 0.0).astype(BF16)
    stacked = jnp.concatenate([both, alone], axis=0)
    step = 4 * HEAD_SIZE

    def twice(ref):
        return jnp.concatenate([ref[...]] * (step // LANES), axis=1)

    for first in range(0, state.shape[2], step):
        spread = dot(stacked, spread_matrix(first // HEAD_SIZE, step))
        block = state[:, :, first : first + step].reshape(rows_all, step)
        new = block * twice(decay_ref) - spread[:rows_all] * twice(removal_ref)
        new = new + spread[rows_all:] * twice(scaled_ref)
        state[:, :, first : first + step] = new.reshape(tokens, HEAD_COUNT, step)

    returned[me] = output[me]

    def ended(number, carry):
        go(number).wait_send()
        copy = back(lax.rem(me + number, total))
        copy.wait_recv()
        copy.wait_send()
        return carry

    lax.fori_loop(1, total, ended, 0)
    routed = dot(coef_ref[...], returned[...].reshape(total * CAP, model))
    hidden_out[...] = (middle_ref[...] + (routed[:tokens] + routed[tokens:])).astype(BF16)

    each_way(lambda copy: copy.wait_send())
    for slot in order[1:]:
        for half in range(UNITS):
            onward(slot, half, lambda copy: copy.wait_send())
    for copy in sent:
        copy.wait_send()
    swap.wait_send()
    exchange.wait_send()


def layer(resid, gain, weights, routes, routing_weight, consts, state, out_w, ffn_gain, experts, ep_size):
    depth = ep_size // PLANE
    chips = ep_size // CORES
    pieces = chips // HEAD_COUNT
    tokens, model = resid.shape
    weights = [w.T for w in weights]
    width = weights[0].shape[0]
    wide = CORES * ROLES * width
    rows_all = tokens * HEAD_COUNT
    routes, routing_weight = routes.T, routing_weight.T
    gain = gain.reshape(model // LANES, LANES)
    ffn_gain = ffn_gain.reshape(model // LANES, LANES)
    consts = [c.reshape(-1, LANES) for c in consts]
    slots = ep_size * CAP
    dma = pltpu.SemaphoreType.DMA
    hbm = pl.BlockSpec(memory_space=pltpu.HBM)
    vmem = pl.BlockSpec(memory_space=pltpu.VMEM)
    operands = (resid, gain, *weights, routes, routing_weight, *consts, state, out_w, ffn_gain, *experts)
    operands = [pltpu.with_memory_space_constraint(a, pltpu.HBM) for a in operands]
    return pl.pallas_call(
        functools.partial(layer_kernel, depth),
        out_shape=(jax.ShapeDtypeStruct((tokens, model), BF16), jax.ShapeDtypeStruct(state.shape, F32)),
        in_specs=[hbm] * len(operands),
        out_specs=(vmem,) * 2,
        scratch_shapes=[
            pltpu.VMEM(gain.shape, BF16),
            pltpu.VMEM((CORES, ROLES, width, model), BF16),
            pltpu.VMEM(routes.shape, jnp.int32),
            pltpu.VMEM(routes.shape, F32),
            pltpu.VMEM((COLUMNS, depth, UNITS, tokens, model // UNITS), BF16),
            pltpu.VMEM((COLUMNS, depth, UNITS, tokens, model // UNITS), BF16),
            pltpu.VMEM((COLUMNS, depth, tokens, wide), BF16),
            pltpu.VMEM((HEAD_COUNT, pieces, tokens, wide), BF16),
            pltpu.VMEM((4,) + consts[0].shape, F32),
            pltpu.VMEM((4, HEAD_COUNT, LANES), F32),
            pltpu.VMEM(out_w.shape, BF16),
            pltpu.VMEM(gain.shape, BF16),
        ]
        + [pltpu.VMEM(w.shape, BF16) for w in experts]
        + [
            pltpu.VMEM((pieces, wide, ROLES * LANES), BF16),
            pltpu.VMEM((ROLES, rows_all, LANES), F32),
        ]
        + [pltpu.VMEM((rows_all, LANES), F32)] * 7
        + [
            pltpu.VMEM((tokens, slots), F32),
            pltpu.VMEM((2 * tokens, slots), BF16),
            pltpu.VMEM((CORES, slots, chips * tokens), BF16),
            pltpu.VMEM((slots, model), BF16),
            pltpu.VMEM((tokens, model), F32),
            pltpu.VMEM((tokens, model), BF16),
        ]
        + [pltpu.VMEM((ep_size, CAP, out_w.shape[0]), BF16)] * 2
        + [pltpu.VMEM((ep_size, CAP, model), BF16)] * 2
        + [
            dma((10,)), dma((ROLES,)), dma((PARTS,)), dma((7,)),
            dma((2, depth, UNITS)), dma((depth, UNITS)),
            dma((2, depth, UNITS)), dma((2, depth, UNITS)),
            dma((depth, UNITS)), dma((depth, UNITS)),
            dma, dma, dma, dma,
            dma((chips,)), dma((chips,)),
        ]
        + [dma((ep_size,))] * 4,
        compiler_params=pltpu.CompilerParams(
            has_side_effects=True, collective_id=0, vmem_limit_bytes=46 * 1024 * 1024
        ),
        cost_estimate=pl.CostEstimate(flops=30_000_000_000, bytes_accessed=100_000_000, transcendentals=0),
    )(*operands)


def store_kernel(state, hidden, next_hbm, hidden_hbm, next_sem, hidden_sem):
    parts = next_sem.shape[0]
    group = state.shape[0] // parts
    copies = [pltpu.make_async_copy(hidden, hidden_hbm, hidden_sem)]
    for part in range(parts):
        here = pl.ds(part * group, group)
        copies.append(pltpu.make_async_copy(state.at[here], next_hbm.at[here], next_sem.at[part]))
    for copy in copies:
        copy.start()
    for copy in copies:
        copy.wait()


def store(state, hidden):
    vmem = pl.BlockSpec(memory_space=pltpu.VMEM)
    hbm = pl.BlockSpec(memory_space=pltpu.HBM)
    dma = pltpu.SemaphoreType.DMA
    return pl.pallas_call(
        store_kernel,
        out_shape=(jax.ShapeDtypeStruct(state.shape, F32), jax.ShapeDtypeStruct(hidden.shape, BF16)),
        in_specs=[vmem] * 2,
        out_specs=(hbm, hbm),
        scratch_shapes=[dma((STORES,)), dma],
        compiler_params=pltpu.CompilerParams(vmem_limit_bytes=4 * 1024 * 1024),
        cost_estimate=pl.CostEstimate(flops=1_000_000_000, bytes_accessed=20_000_000, transcendentals=0),
    )(state, hidden)


def per_device(
    residual_input,
    attention_norm_gain,
    receptance_weight,
    key_weight,
    value_weight,
    decay_weight,
    correction_rate_weight,
    output_gate_weight,
    decay_offset,
    correction_rate_offset,
    self_term_weight,
    head_read_gain,
    previous_state,
    attention_output_weight,
    feedforward_norm_gain,
    routes,
    routing_weight,
    routed_gate_weight,
    routed_up_weight,
    routed_down_weight,
    common_gate_weight,
    common_up_weight,
    common_down_weight,
):
    ep_size = lax.axis_size("ep")
    hidden, state = layer(
        residual_input,
        attention_norm_gain,
        (
            receptance_weight,
            key_weight,
            value_weight,
            decay_weight,
            correction_rate_weight,
            output_gate_weight,
        ),
        routes,
        routing_weight,
        (decay_offset, correction_rate_offset, self_term_weight, head_read_gain),
        previous_state,
        attention_output_weight,
        feedforward_norm_gain,
        (
            common_gate_weight,
            common_up_weight,
            common_down_weight,
            routed_gate_weight[0],
            routed_up_weight[0],
            routed_down_weight[0],
        ),
        ep_size,
    )
    next_state, hidden_out = store(state, hidden)
    return (hidden_out, next_state)


def solution(mesh):
    return jax.shard_map(
        per_device,
        mesh=mesh,
        in_specs=(
            P(("grp", "ep"), None),
            P(),
            P(None, "ep"),
            P(None, "ep"),
            P(None, "ep"),
            P(None, "ep"),
            P(None, "ep"),
            P(None, "ep"),
            P(),
            P(),
            P(),
            P(),
            P(("grp", "ep"), None, None),
            P(),
            P(),
            P("grp", None),
            P("grp", None),
            P("ep", None, None),
            P("ep", None, None),
            P("ep", None, None),
            P(),
            P(),
            P(),
        ),
        out_specs=(P(("grp", "ep"), None), P(("grp", "ep"), None, None)),
        check_vma=False,
    )
```
